32 devices in a mesh: grp: 2 (over y), sp: 4 (over z), tp: 4 (over x, core).
Axes of the slice: x: 2, y: 2, z: 4, core: 2. Of those that a mesh axis runs over, the one named last changes fastest.
Arguments:
- hidden: bfloat16 [3072, 2048], P(('grp', 'sp'), 'tp'), parts along dimension 0, may hold values from -45 to 45
- norm_gain: bfloat16 [2048], replicated, may hold values from 0.099609375 to 1.8984375
- w_query: bfloat16 [2048, 1024], P(None, 'tp'), may hold values from -0.125 to 0.125
- w_key: bfloat16 [2048, 1024], P(None, 'tp'), may hold values from -0.125 to 0.125
- w_value: bfloat16 [2048, 1024], P(None, 'tp'), may hold values from -0.125 to 0.125
- query_gain: float32 [8, 128], P('tp'), may hold values from 0.3 to 16
- key_gain: float32 [8, 128], P('tp'), may hold values from 0.3 to 16
- w_out: bfloat16 [1024, 2048], P('tp'), may hold values from -1.5 to 1.5
Outputs:
- mixed: bfloat16 [3072, 2048], P(('grp', 'sp'), 'tp'), parts along dimension 0
- log_total: float32 [3072, 8], P(('grp', 'sp'), 'tp'), parts along dimension 0
The draws below stay inside these ranges and needn't reach their ends.
There are 2 independent parts, one for each index of `grp`. The reference program is written for one: setup_inputs(seed, part) draws one part's arguments, and reference() takes and returns one part's arrays. A program takes and returns all parts, laid end to end along the dimension named above; an argument that names none is the same for every part. Nothing has to cross between parts.
All inputs are finite; a program needn't handle non-finite values.
Results may differ from the reference program's by a relative error of at most 0.015.
The reference program's roundings to bfloat16 on the way count: a program that leaves them out, or rounds other values in their place, can miss the bound.
Values may be sent and summed in bfloat16 or wider, within the bound.
A program may use at most 64 MiB of HBM per device.

```python
import jax
import jax.numpy as jnp
from jax import lax

D = 2048
HEADS = 8
HEAD_DIM = 128
KEYS_BEHIND = 128
MIDDLE_DILATION = 4
WIDEST_DILATION = 16
TOKENS = 1536


def draw_hidden(key, part):
    row_key, col_key, base_key = jax.random.split(jax.random.fold_in(key, 17), 3)
    row_factor = jnp.exp(jax.random.uniform(row_key, (TOKENS, 1), jnp.float32, -1.2, 1.1))
    rising = 1.0 + 2.0 * jnp.arange(D, dtype=jnp.float32) / D
    col_factor = jnp.exp(jax.random.uniform(col_key, (1, D), jnp.float32, 0.0, 2.3)) * rising * 0.125
    base = jnp.clip(jax.random.normal(base_key, (TOKENS, D), jnp.float32), -4.0, 4.0)
    return (base * row_factor * col_factor).astype(jnp.bfloat16)


def head_gains(key, salt):
    channel_key = jax.random.fold_in(jax.random.fold_in(key, salt), 1)
    noise = jnp.clip(jax.random.normal(channel_key, (HEADS, HEAD_DIM), jnp.float32), -3.5, 3.5)
    return (1.0 + 0.18 * noise).astype(jnp.float32)


def draw_query_gain(key, part):
    return head_gains(key, 31)


def draw_key_gain(key, part):
    return head_gains(key, 47)


def block_levels(stream_key, shape, pieces, low, high):
    factor_of = 1.0
    for dim, parts in pieces:
        draws = jax.random.uniform(jax.random.fold_in(jax.random.fold_in(stream_key, 6), dim), (parts,), jnp.float32, low / len(pieces), high / len(pieces))
        factor_of = factor_of * jnp.repeat(jnp.exp(draws), shape[dim] // parts).reshape((-1,) + (1,) * (len(shape) - 1 - dim))
    return factor_of


def centred(key, dims, scale, bound, cuts=(), held_as=jnp.bfloat16):
    drawn = jax.random.normal(key, dims, jnp.float32) * scale
    if len(cuts) > 0:
        drawn = block_levels(key, dims, cuts, -0.22, 0.18) * drawn
    return jnp.clip(drawn, min=-bound, max=bound).astype(held_as)


def setup_inputs(seed: int = 0, part: int = 0) -> dict:
    seeds = jax.random.split(jax.random.key(seed), 9)
    part_splits = jax.random.split(jax.random.fold_in(seeds[8], part), 9)
    return {
        "hidden": draw_hidden(jax.random.fold_in(jax.random.fold_in(seeds[8], part), 71), part),
        "norm_gain": jnp.clip(1.0 + 0.18 * jax.random.normal(seeds[1], (D,), jnp.float32), 0.099609375, 1.8984375).astype(jnp.bfloat16),
        "w_query": centred(seeds[2], (D, HEADS * HEAD_DIM), D ** -0.5, 0.125, ((1, 4),)),
        "w_key": centred(seeds[3], (D, HEADS * HEAD_DIM), D ** -0.5, 0.125, ((1, 4),)),
        "w_value": centred(seeds[4], (D, HEADS * HEAD_DIM), D ** -0.5, 0.125, ((1, 4),)),
        "query_gain": draw_query_gain(jax.random.fold_in(seeds[8], 71), part),
        "key_gain": draw_key_gain(jax.random.fold_in(seeds[8], 71), part),
        "w_out": centred(seeds[7], (HEADS * HEAD_DIM, D), 16 ** -0.5, 1.5, ((0, 4),)),
    }


EPSILON = 1e-06
ROTARY_BASE = 500000.0

def rotate(values, positions):
    head_width = values.shape[-1]
    inverse = ROTARY_BASE ** (-jnp.arange(0, head_width, 2, dtype=jnp.float32) / head_width)
    angles = positions[:, None] * inverse[None, :]
    cosine = jnp.cos(angles)[:, None, :]
    sine = jnp.sin(angles)[:, None, :]
    half_width = head_width // 2
    first_half = values[..., :half_width]
    second_half = values[..., half_width:]
    return jnp.concatenate([first_half * cosine - second_half * sine, second_half * cosine + first_half * sine], axis=-1)

def head_norm(values, gains):
    normed = values * lax.rsqrt(lax.optimization_barrier(jnp.mean(values * values, axis=-1, keepdims=True)) + EPSILON)
    return normed * gains[None, :, :]

def dilated_branch(query, key_all, value_all, dilation_step):
    sequence_rows, head_count, head_width = query.shape
    class_rows = sequence_rows // dilation_step
    block_count = -(-class_rows // KEYS_BEHIND)
    padded_rows = block_count * KEYS_BEHIND

    def by_class(values):
        return values.reshape(class_rows, dilation_step, head_count, head_width).transpose(1, 0, 2, 3).astype(jnp.float32)
    query_blocks = jnp.pad(by_class(query), ((0, 0), (0, padded_rows - class_rows), (0, 0), (0, 0)))
    query_blocks = query_blocks.reshape(dilation_step, block_count, KEYS_BEHIND, head_count, head_width)

    def windows(values):
        padded = jnp.pad(by_class(values), ((0, 0), (KEYS_BEHIND, padded_rows - class_rows), (0, 0), (0, 0)))
        padded = padded.reshape(dilation_step, block_count + 1, KEYS_BEHIND, head_count, head_width)
        return jnp.concatenate([padded[:, :-1], padded[:, 1:]], axis=2)
    key_windows = windows(key_all)
    value_windows = windows(value_all)
    scores = jnp.einsum('rnqhd,rnkhd->rnhqk', query_blocks, key_windows) * head_width ** (-0.5)
    row_index = jnp.arange(KEYS_BEHIND, dtype=jnp.int32)[:, None]
    col_index = jnp.arange(2 * KEYS_BEHIND, dtype=jnp.int32)[None, :]
    distance = row_index + KEYS_BEHIND - col_index
    in_band = (distance >= 0) & (distance <= KEYS_BEHIND)
    class_index = jnp.arange(block_count, dtype=jnp.int32)[:, None] * KEYS_BEHIND + col_index - KEYS_BEHIND
    allowed = in_band[None, :, :] & (class_index >= 0)[:, None, :]
    scores = jnp.where(allowed[None, :, None, :, :], scores, -jnp.inf)
    row_max = lax.optimization_barrier(jnp.max(scores, axis=-1, keepdims=True))
    weights = jnp.exp(scores - row_max)
    weight_sum = lax.optimization_barrier(jnp.sum(weights, axis=-1))
    rounded = lax.optimization_barrier(weights.astype(jnp.bfloat16)).astype(jnp.float32)
    weighted = jnp.einsum('rnhqk,rnkhd->rnqhd', rounded, value_windows)
    branch_out = weighted / jnp.transpose(weight_sum, (0, 1, 3, 2))[..., None]
    branch_out = branch_out.reshape(dilation_step, padded_rows, head_count, head_width)[:, :class_rows]
    branch_out = branch_out.transpose(1, 0, 2, 3).reshape(sequence_rows, head_count, head_width)
    log_sum = jnp.transpose(row_max[..., 0] + jnp.log(weight_sum), (0, 1, 3, 2))
    log_sum = log_sum.reshape(dilation_step, padded_rows, head_count)[:, :class_rows]
    log_sum = log_sum.transpose(1, 0, 2).reshape(sequence_rows, head_count)
    return (branch_out, log_sum)

def reference(hidden, norm_gain, w_query, w_key, w_value, query_gain, key_gain, w_out):
    sequence_rows = hidden.shape[0]
    hidden_float = hidden.astype(jnp.float32)
    row_scale = lax.rsqrt(lax.optimization_barrier(jnp.mean(hidden_float * hidden_float, axis=1, keepdims=True)) + EPSILON)
    scaled = (hidden_float * norm_gain.astype(jnp.float32)[None, :]).astype(jnp.bfloat16)
    query_raw = jnp.dot(scaled, w_query, preferred_element_type=jnp.float32) * row_scale
    key_raw = jnp.dot(scaled, w_key, preferred_element_type=jnp.float32) * row_scale
    value_raw = jnp.dot(scaled, w_value, preferred_element_type=jnp.float32) * row_scale
    positions = jnp.arange(sequence_rows, dtype=jnp.int32).astype(jnp.float32)
    query = rotate(head_norm(query_raw.reshape(sequence_rows, HEADS, HEAD_DIM), query_gain), positions).astype(jnp.bfloat16)
    key_all = rotate(head_norm(key_raw.reshape(sequence_rows, HEADS, HEAD_DIM), key_gain), positions).astype(jnp.bfloat16)
    value_all = value_raw.astype(jnp.bfloat16).reshape(sequence_rows, HEADS, HEAD_DIM)
    branch_outs = []
    branch_logs = []
    for dilation_step in (1, MIDDLE_DILATION, WIDEST_DILATION):
        branch_out, log_sum = dilated_branch(query, key_all, value_all, dilation_step)
        branch_outs.append(branch_out)
        branch_logs.append(log_sum)
    stacked_logs = jnp.stack(branch_logs, axis=0)
    peak = lax.optimization_barrier(jnp.max(stacked_logs, axis=0))
    log_total = peak + jnp.log(lax.optimization_barrier(jnp.sum(jnp.exp(stacked_logs - peak[None]), axis=0)))
    shares = jnp.exp(stacked_logs - log_total[None])
    attended = lax.optimization_barrier(jnp.sum(shares[..., None] * jnp.stack(branch_outs, axis=0), axis=0))
    attended = attended.astype(jnp.bfloat16).reshape(sequence_rows, HEADS * HEAD_DIM)
    mixed = jnp.dot(attended, w_out, preferred_element_type=jnp.float32).astype(jnp.bfloat16)
    return (mixed, log_total)
```

```python
import functools
import math

import jax
import jax.numpy as jnp
import numpy as np
from jax import lax
from jax.experimental import pallas as pl
from jax.experimental.pallas import tpu as pltpu
from jax.sharding import PartitionSpec as P

D = 2048
KEYS_BEHIND = 128
MIDDLE_DILATION = 4
WIDEST_DILATION = 16


EPSILON = 1e-06
ROTARY_BASE = 500000.0


def from_behind(value, axis, steps):
    count = lax.axis_size(axis)
    initial, last = (max(0, -steps), min(count, count - steps))
    return lax.ppermute(value, axis, [(source, source + steps) for source in range(initial, last)])


def rotate(values, positions):
    head_width = values.shape[-1]
    inverse = ROTARY_BASE ** (-jnp.arange(0, head_width, 2, dtype=jnp.float32) / head_width)
    angles = positions[:, None] * inverse[None, :]
    cosine = jnp.cos(angles)[:, None, :]
    sine = jnp.sin(angles)[:, None, :]
    half_width = head_width // 2
    first_half = values[..., :half_width]
    second_half = values[..., half_width:]
    return jnp.concatenate(
        [first_half * cosine - second_half * sine, second_half * cosine + first_half * sine],
        axis=-1,
    )


def head_norm(values, gains):
    normed = values * lax.rsqrt(jnp.mean(values * values, axis=-1, keepdims=True) + EPSILON)
    return normed * gains[None, :, :]


def earlier_pairs(own_pair, token_rows):
    distant_shards = (KEYS_BEHIND * WIDEST_DILATION + token_rows - 1) // token_rows
    pieces = [own_pair]
    for distance in range(1, distant_shards + 1):
        pieces.insert(0, from_behind(own_pair, "sp", distance))
    buffer = jnp.concatenate(pieces, axis=1)
    return buffer


def local_branch(query, key_rows, value_rows, dilation_step, first_pos):
    token_rows, head_count, head_width = query.shape
    reach_rows = KEYS_BEHIND * dilation_step
    buffer_rows = key_rows.shape[0]
    class_rows = token_rows // dilation_step
    class_keys = class_rows + KEYS_BEHIND
    window_start = buffer_rows - token_rows - reach_rows
    key_window = key_rows[window_start:]
    value_window = value_rows[window_start:]
    query_class = query.reshape(class_rows, dilation_step, head_count, head_width).transpose(
        1, 0, 2, 3
    )
    key_class = key_window.reshape(class_keys, dilation_step, head_count, head_width).transpose(
        1, 0, 2, 3
    )
    value_class = value_window.reshape(class_keys, dilation_step, head_count, head_width).transpose(
        1, 0, 2, 3
    )
    block_rows = math.gcd(class_rows, KEYS_BEHIND) if class_rows > KEYS_BEHIND else class_rows
    block_count = class_rows // block_rows
    query_blocks = query_class.reshape(
        dilation_step, block_count, block_rows, head_count, head_width
    )
    key_blocks = jnp.stack(
        [
            key_class[:, number * block_rows : number * block_rows + block_rows + KEYS_BEHIND]
            for number in range(block_count)
        ],
        axis=1,
    )
    value_blocks = jnp.stack(
        [
            value_class[:, number * block_rows : number * block_rows + block_rows + KEYS_BEHIND]
            for number in range(block_count)
        ],
        axis=1,
    )
    scores = jnp.einsum(
        "rnqhd,rnkhd->rnhqk", query_blocks, key_blocks, preferred_element_type=jnp.float32
    ) * head_width ** (-0.5)
    row_index = jnp.arange(block_rows, dtype=jnp.int32)[:, None]
    col_index = jnp.arange(block_rows + KEYS_BEHIND, dtype=jnp.int32)[None, :]
    distance = KEYS_BEHIND + row_index - col_index
    in_band = (distance >= 0) & (distance <= KEYS_BEHIND)
    class_index = jnp.arange(block_count, dtype=jnp.int32)[:, None] * block_rows + col_index
    residue = jnp.arange(dilation_step, dtype=jnp.int32)[:, None, None]
    key_position = first_pos - reach_rows + class_index[None] * dilation_step + residue
    allowed = in_band[None, None, None, :, :] & (key_position >= 0)[:, :, None, None, :]
    scores = jnp.where(allowed, scores, -jnp.inf)
    row_max = jnp.max(scores, axis=-1, keepdims=True)
    weights = jnp.exp(scores - row_max)
    weight_sum = jnp.sum(weights, axis=-1)
    weighted = jnp.einsum(
        "rnhqk,rnkhd->rnqhd",
        weights.astype(jnp.bfloat16),
        value_blocks,
        preferred_element_type=jnp.float32,
    )
    branch_out = weighted / jnp.transpose(weight_sum, (0, 1, 3, 2))[..., None]
    branch_out = branch_out.reshape(dilation_step, class_rows, head_count, head_width).transpose(
        1, 0, 2, 3
    )
    branch_out = branch_out.reshape(token_rows, head_count, head_width)
    log_sum = jnp.transpose(row_max[..., 0] + jnp.log(weight_sum), (0, 1, 3, 2))
    log_sum = (
        log_sum.reshape(dilation_step, class_rows, head_count)
        .transpose(1, 0, 2)
        .reshape(token_rows, head_count)
    )
    return (branch_out, log_sum)


def local(hidden, norm_gain, w_query, w_key, w_value, query_gain, key_gain, w_out):
    token_rows = hidden.shape[0]
    local_width = w_query.shape[1]
    head_count = query_gain.shape[0]
    head_width = query_gain.shape[1]
    gain_full = norm_gain.astype(jnp.float32)
    raw_piece = lax.all_gather(hidden, "tp", axis=1, tiled=True).astype(jnp.float32)
    scaled = (raw_piece * gain_full[None, :]).astype(jnp.bfloat16)

    def add_product(weight):
        return jnp.dot(scaled, weight, preferred_element_type=jnp.float32)

    query_raw = add_product(w_query)
    key_raw = add_product(w_key)
    value_raw = add_product(w_value)
    squares = jnp.sum(raw_piece * raw_piece, axis=1)
    row_scale = lax.rsqrt(squares / D + EPSILON)[:, None]
    first_pos = lax.axis_index("sp") * token_rows
    positions = (jnp.arange(token_rows, dtype=jnp.int32) + first_pos).astype(jnp.float32)
    query = rotate(
        head_norm((query_raw * row_scale).reshape(token_rows, head_count, head_width), query_gain),
        positions,
    ).astype(jnp.bfloat16)
    key_now = rotate(
        head_norm((key_raw * row_scale).reshape(token_rows, head_count, head_width), key_gain),
        positions,
    ).astype(jnp.bfloat16)
    value_now = (value_raw * row_scale).astype(jnp.bfloat16)
    own_pair = jnp.stack([key_now.reshape(token_rows, local_width), value_now], axis=0)
    buffer = earlier_pairs(own_pair, token_rows)
    key_rows = buffer[0].reshape(-1, head_count, head_width)
    value_rows = buffer[1].reshape(-1, head_count, head_width)
    branch_outs = []
    branch_logs = []
    for dilation_step in (1, MIDDLE_DILATION, WIDEST_DILATION):
        branch_out, log_sum = local_branch(query, key_rows, value_rows, dilation_step, first_pos)
        branch_outs.append(branch_out)
        branch_logs.append(log_sum)
    stacked_logs = jnp.stack(branch_logs, axis=0)
    peak = jnp.max(stacked_logs, axis=0)
    log_total = peak + jnp.log(jnp.sum(jnp.exp(stacked_logs - peak[None]), axis=0))
    shares = jnp.exp(stacked_logs - log_total[None])
    attended = jnp.sum(shares[..., None] * jnp.stack(branch_outs, axis=0), axis=0)
    attended = attended.astype(jnp.bfloat16).reshape(token_rows, local_width)
    column_block = lax.all_to_all(w_out, "tp", split_axis=1, concat_axis=0, tiled=True)
    mixed = jnp.dot(
        lax.all_gather(attended, "tp", axis=1, tiled=True),
        column_block,
        preferred_element_type=jnp.float32,
    )
    return (mixed.astype(jnp.bfloat16), log_total)


MESH = pl.DeviceIdType.MESH
LANES = 128


def rotary_table(classes, rows, head_width):
    inverse = (ROTARY_BASE ** (-np.arange(0, head_width, 2, dtype=np.float64) / head_width)).astype(np.float32)
    positions = np.arange(classes * classes * rows, dtype=np.float32)
    angles = (positions[:, None] * inverse[None, :]).astype(np.float64)
    cosine, sine = np.cos(angles), np.sin(angles)
    table = np.concatenate([cosine, cosine, -sine, sine], axis=1).astype(np.float32)
    return table.reshape(classes, rows, classes, 2 * head_width).transpose(0, 2, 1, 3)


def class_kernel(
    hid_ref, gain_ref, qgain_ref, kgain_ref, wq_ref, wk_ref, wv_ref, wo_ref, table_ref,
    mixed_ref, total_ref,
    hb, hc, wall, wo, tb, tc, acc_b, acc_c, q_b, kv_b, kv_c, q_c, halo, oc, lsend, ro, rl, at,
    loc, zs, zr, axs, axr, acs, acr, afs, afr, cxs, cxr, ccs, ccr, cfs, cfr,
    wos, wor, hs, hr, rs, rr, ls, lr, gxs, gxr, gcs, gcr, gfs, gfr,
):
    f32, bf16 = jnp.float32, jnp.bfloat16
    s, p = lax.axis_index("sp"), lax.axis_index("tp")
    n = MIDDLE_DILATION
    rows, width = hid_ref.shape
    sub = rows // n
    heads, hd = qgain_ref.shape
    lw = heads * hd
    halo_sub = halo.shape[1]
    halo_rows = n * halo_sub
    core = p + 1 - 2 * lax.rem(p, 2)
    xp = lax.rem(p + 2, 4)
    diag = lax.rem(core + 2, 4)

    def tp_copy(src, dst, ss, sr, q):
        return pltpu.make_async_remote_copy(
            src_ref=src, dst_ref=dst, send_sem=ss, recv_sem=sr, device_id={"tp": q}, device_id_type=MESH
        )

    def sp_copy(src, dst, ss, sr, q):
        return pltpu.make_async_remote_copy(
            src_ref=src, dst_ref=dst, send_sem=ss, recv_sem=sr, device_id={"sp": q}, device_id_type=MESH
        )

    barrier = pltpu.get_barrier_semaphore()
    for q in (core, xp, diag):
        pl.semaphore_signal(barrier, inc=1, device_id={"tp": q}, device_id_type=MESH)
    for k in range(1, n):
        pl.semaphore_signal(barrier, inc=1, device_id={"sp": lax.rem(s + k, n)}, device_id_type=MESH)
    loads = [
        pltpu.make_async_copy(wq_ref, wall.at[:, pl.ds(0, lw)], loc.at[0]),
        pltpu.make_async_copy(wk_ref, wall.at[:, pl.ds(lw, lw)], loc.at[1]),
        pltpu.make_async_copy(wv_ref, wall.at[:, pl.ds(2 * lw, lw)], loc.at[2]),
        pltpu.make_async_copy(table_ref.at[s], tb, loc.at[3]),
        pltpu.make_async_copy(table_ref.at[:, s], tc, loc.at[4]),
        pltpu.make_async_copy(
            wo_ref.at[:, pl.ds(pl.multiple_of(p * width, LANES), width)], wo.at[p], loc.at[5]
        ),
    ]
    for load in loads:
        load.start()

    def iota(shape, dim):
        return lax.broadcasted_iota(jnp.int32, shape, dim)

    def row_of(r, part):
        return n * lax.rem(r, part) + r // part

    square = (rows, rows)
    to_class = (row_of(iota(square, 0), sub) == iota(square, 1)).astype(f32).astype(bf16)
    permuted = jnp.dot(to_class, hid_ref[...], preferred_element_type=f32).astype(bf16)
    hb[p] = permuted.reshape(n, sub, width)
    hc[p, s] = hb[p, s]
    pl.semaphore_wait(barrier, 3 + n - 1)

    sends = []

    def go(copy):
        copy.start()
        sends.append(copy)
        return copy

    za = [None] + [
        go(sp_copy(hb.at[p, lax.rem(s + k, n)], hc.at[p, s], zs.at[k], zr.at[k], lax.rem(s + k, n)))
        for k in range(1, n)
    ]
    ax = [go(tp_copy(hb.at[p, i], hb.at[p, i], axs.at[i], axr.at[i], xp)) for i in range(n)]
    ac = go(tp_copy(hb.at[p], hb.at[p], acs, acr, core))

    block_of = [lax.rem(s + n - k, n) for k in range(n)]
    cx, cc = [], []

    def spread(k):
        piece = hc.at[p, block_of[k]]
        cx.append(go(tp_copy(piece, piece, cxs.at[k], cxr.at[k], xp)))
        cc.append(go(tp_copy(piece, piece, ccs.at[k], ccr.at[k], core)))

    spread(0)

    def chunk(source, q):
        raw = source[q].reshape(rows, width).astype(f32)
        scaled = (raw * gain_ref[q]).astype(bf16)
        w = wall[pl.ds(pl.multiple_of(q * width, LANES), width), :]
        return jnp.dot(scaled, w, preferred_element_type=f32), jnp.sum(raw * raw, axis=1, keepdims=True)

    for load in loads:
        load.wait()
    acc_b[...], sq_b = chunk(hb, p)
    ac.wait_recv()
    prod, more = chunk(hb, core)
    acc_b[...] += prod
    sq_b += more

    af = []
    for i in range(n):
        ax[i].wait_recv()
        af.append(go(tp_copy(hb.at[xp, i], hb.at[xp, i], afs.at[i], afr.at[i], core)))
        if i >= 1:
            za[i].wait_recv()
            spread(i)
    w_sends = []
    for j, q in enumerate((core, xp, diag)):
        w_sends.append(
            go(tp_copy(wo_ref.at[:, pl.ds(pl.multiple_of(q * width, LANES), width)], wo.at[p], wos.at[j], wor.at[j], q))
        )

    prod, more = chunk(hb, xp)
    acc_b[...] += prod
    sq_b += more
    for copy in af:
        copy.wait_recv()
    prod, more = chunk(hb, diag)
    sq_b += more

    def finish(acc, sq, table, q_out, kv_out):
        raw = acc * lax.rsqrt(sq / (width * 4) + EPSILON)
        table = table[...].reshape(rows, 2 * hd)
        cosine, sine = table[:, :hd], table[:, hd:]
        for h in range(heads):
            for start, gains, out in ((0, qgain_ref, q_out), (lw, kgain_ref, kv_out)):
                x = raw[:, start + h * hd : start + (h + 1) * hd]
                x = x * lax.rsqrt(jnp.mean(x * x, axis=-1, keepdims=True) + EPSILON)
                x = x * gains[pl.ds(h, 1), :]
                x = x * cosine + pltpu.roll(x, hd // 2, 1) * sine
                out[:, :, h * hd : (h + 1) * hd] = x.astype(bf16).reshape(n, sub, hd)
        kv_out[:, :, lw:] = raw[:, 2 * lw :].astype(bf16).reshape(n, sub, lw)

    finish(acc_b[...] + prod, sq_b, tb, q_b, kv_b)
    halo_send = sp_copy(kv_b.at[:, pl.ds(sub - halo_sub, halo_sub), :], halo, hs, hr, lax.rem(s + 1, n))

    @pl.when(s < n - 1)
    def _():
        halo_send.start()

    @pl.when(s == 0)
    def _():
        halo[...] = jnp.zeros_like(halo)

    cf = []
    for k in range(n):
        cx[k].wait_recv()
        piece = hc.at[xp, block_of[k]]
        cf.append(go(tp_copy(piece, piece, cfs.at[k], cfr.at[k], core)))
        if k == n - 2:
            for copy in cc:
                copy.wait_recv()
            prod, sq_c = chunk(hc, p)
            prod2, more = chunk(hc, core)
            acc_c[...] = prod + prod2
            sq_c += more
    prod, more = chunk(hc, xp)
    acc_c[...] += prod
    sq_c += more
    for copy in cf:
        copy.wait_recv()
    prod, more = chunk(hc, diag)
    sq_c += more
    finish(acc_c[...] + prod, sq_c, tc, q_c, kv_c)

    def attend(q, k, v, bias):
        score = lax.dot_general(q, k, (((1,), (1,)), ((), ())), preferred_element_type=f32)
        score = score * hd ** (-0.5) + bias
        top = jnp.max(score, axis=-1, keepdims=True)
        weight = jnp.exp(score - top)
        total = jnp.sum(weight, axis=-1, keepdims=True)
        out = jnp.dot(weight.astype(bf16), v, preferred_element_type=f32) / total
        return out, top + jnp.log(total)

    behind = iota(square, 0) - iota(square, 1)
    stride = WIDEST_DILATION // n
    near = (behind >= 0) & (behind <= KEYS_BEHIND)
    far = (behind >= 0) & (behind <= KEYS_BEHIND * stride) & ((behind + rows * stride) % stride == 0)
    bias_c = jnp.where(
        near & far, math.log(2.0), jnp.where(near | far, 0.0, -jnp.inf)
    ).astype(f32)
    lane = iota((rows, LANES), 1)
    logs = jnp.zeros((rows, LANES), f32)
    for h in range(heads):
        cols = slice(h * hd, (h + 1) * hd)
        vcols = slice(lw + h * hd, lw + (h + 1) * hd)
        out, lse = attend(
            q_c[:, :, cols].reshape(rows, hd), kv_c[:, :, cols].reshape(rows, hd),
            kv_c[:, :, vcols].reshape(rows, hd), bias_c,
        )
        oc[:, :, cols] = out.astype(bf16).reshape(n, sub, hd)
        logs = jnp.where(lane == h, lse, logs)
    pad = LANES - sub
    for b in range(n):
        part = jnp.concatenate([logs[b * sub : (b + 1) * sub], jnp.zeros((pad, LANES), f32)], axis=0)
        lsend[b] = jnp.transpose(part)[:8]
    back, back_l = [], []
    for k in range(1, n):
        to = lax.rem(s + k, n)
        back.append(go(sp_copy(oc.at[to], ro.at[s], rs.at[k], rr.at[k], to)))
        back_l.append(go(sp_copy(lsend.at[to], rl.at[s], ls.at[k], lr.at[k], to)))
    ro[s] = oc[s]
    rl[s] = lsend[s]

    @pl.when(s > 0)
    def _():
        halo_send.wait_recv()

    total_keys = rows + halo_rows
    wide = (rows, total_keys)
    key = iota(wide, 1)
    key_row = jnp.where(key < rows, row_of(key, sub), row_of(key - rows, halo_sub) - halo_rows)
    behind = row_of(iota(wide, 0), sub) - key_row
    ok = (behind >= 0) & (behind <= KEYS_BEHIND) & (key_row + s * rows >= 0)
    bias_b = jnp.where(ok, 0.0, -jnp.inf).astype(f32)
    near_parts = []
    for h in range(heads):
        cols = slice(h * hd, (h + 1) * hd)
        vcols = slice(lw + h * hd, lw + (h + 1) * hd)
        near_parts.append(attend(
            q_b[:, :, cols].reshape(rows, hd),
            jnp.concatenate([kv_b[:, :, cols].reshape(rows, hd), halo[:, :, cols].reshape(halo_rows, hd)], axis=0),
            jnp.concatenate([kv_b[:, :, vcols].reshape(rows, hd), halo[:, :, vcols].reshape(halo_rows, hd)], axis=0),
            bias_b,
        ))

    for copy in back + back_l:
        copy.wait_recv()
    far_logs = jnp.concatenate(
        [
            jnp.transpose(jnp.concatenate([rl[i], jnp.zeros((LANES - 8, LANES), f32)], axis=0))[:sub]
            for i in range(n)
        ],
        axis=0,
    )
    logs = jnp.zeros((rows, LANES), f32)
    mixed_heads = []
    for h in range(heads):
        out, lse = near_parts[h]
        far_lse = far_logs[:, h : h + 1]
        far_out = ro[:, :, h * hd : (h + 1) * hd].reshape(rows, hd).astype(f32)
        top = jnp.maximum(lse, far_lse)
        e_near, e_far = jnp.exp(lse - top), jnp.exp(far_lse - top)
        both = e_near + e_far
        logs = jnp.where(lane == h, top + jnp.log(both), logs)
        mixed_heads.append(((e_near * out + e_far * far_out) / both).astype(bf16))
    attended = jnp.concatenate(mixed_heads, axis=1)
    from_class = (iota(square, 0) == row_of(iota(square, 1), sub)).astype(f32).astype(bf16)
    at[p] = jnp.dot(from_class, attended, preferred_element_type=f32).astype(bf16)
    half = rows // 2
    gx = [
        go(tp_copy(at.at[p, pl.ds(i * half, half)], at.at[p, pl.ds(i * half, half)], gxs.at[i], gxr.at[i], xp))
        for i in range(2)
    ]
    gc = go(tp_copy(at.at[p], at.at[p], gcs, gcr, core))
    high = logs.astype(bf16)
    rest = logs - high.astype(f32)
    middle = rest.astype(bf16)
    low = (rest - middle.astype(f32)).astype(bf16)
    ordered = sum(jnp.dot(from_class, x, preferred_element_type=f32) for x in (high, middle, low))
    total_ref[...] = ordered[:, :heads]

    result = jnp.dot(at[p], wo[p], preferred_element_type=f32)
    for copy in w_sends:
        copy.wait_recv()
    gc.wait_recv()
    result += jnp.dot(at[core], wo[core], preferred_element_type=f32)
    gf = []
    for i in range(2):
        gx[i].wait_recv()
        piece = at.at[xp, pl.ds(i * half, half)]
        gf.append(go(tp_copy(piece, piece, gfs.at[i], gfr.at[i], core)))
    result += jnp.dot(at[xp], wo[xp], preferred_element_type=f32)
    for copy in gf:
        copy.wait_recv()
    result += jnp.dot(at[diag], wo[diag], preferred_element_type=f32)
    mixed_ref[...] = result.astype(bf16)
    for copy in sends:
        copy.wait_send()

    @pl.when(s < n - 1)
    def _():
        halo_send.wait_send()


def local_by_class(hidden, norm_gain, w_query, w_key, w_value, query_gain, key_gain, w_out):
    n = MIDDLE_DILATION
    rows, width = hidden.shape
    heads, hd = query_gain.shape
    lw = heads * hd
    sub = rows // n
    halo_sub = KEYS_BEHIND // n
    bf16, f32 = jnp.bfloat16, jnp.float32
    table = jnp.asarray(rotary_table(n, sub, hd))
    vmem = pl.BlockSpec(memory_space=pltpu.VMEM)
    anyspace = pl.BlockSpec(memory_space=pl.ANY)
    dma = pltpu.SemaphoreType.DMA
    return pl.pallas_call(
        class_kernel,
        out_shape=(
            jax.ShapeDtypeStruct((rows, w_out.shape[1] // 4), bf16),
            jax.ShapeDtypeStruct((rows, heads), f32),
        ),
        in_specs=[vmem] * 4 + [anyspace] * 5,
        out_specs=(vmem, vmem),
        scratch_shapes=[
            pltpu.VMEM((4, n, sub, width), bf16),
            pltpu.VMEM((4, n, sub, width), bf16),
            pltpu.VMEM((4 * width, 3 * lw), bf16),
            pltpu.VMEM((4, lw, width), bf16),
            pltpu.VMEM((n, sub, 2 * hd), f32),
            pltpu.VMEM((n, sub, 2 * hd), f32),
            pltpu.VMEM((rows, 3 * lw), f32),
            pltpu.VMEM((rows, 3 * lw), f32),
            pltpu.VMEM((n, sub, lw), bf16),
            pltpu.VMEM((n, sub, 2 * lw), bf16),
            pltpu.VMEM((n, sub, 2 * lw), bf16),
            pltpu.VMEM((n, sub, lw), bf16),
            pltpu.VMEM((n, halo_sub, 2 * lw), bf16),
            pltpu.VMEM((n, sub, lw), bf16),
            pltpu.VMEM((n, 8, LANES), f32),
            pltpu.VMEM((n, sub, lw), bf16),
            pltpu.VMEM((n, 8, LANES), f32),
            pltpu.VMEM((4, rows, lw), bf16),
            dma((6,)),
            dma((n,)), dma((n,)),
            dma((n,)), dma((n,)), dma, dma, dma((n,)), dma((n,)),
            dma((n,)), dma((n,)), dma((n,)), dma((n,)), dma((n,)), dma((n,)),
            dma((3,)), dma((3,)),
            dma, dma,
            dma((n,)), dma((n,)), dma((n,)), dma((n,)),
            dma((2,)), dma((2,)), dma, dma, dma((2,)), dma((2,)),
        ],
        compiler_params=pltpu.CompilerParams(
            collective_id=0, has_side_effects=True, vmem_limit_bytes=60 * 1024 * 1024
        ),
    )(
        hidden, norm_gain.astype(f32).reshape(4, 1, width), query_gain, key_gain,
        w_query, w_key, w_value, w_out, table,
    )


def solution(mesh):
    split = mesh.shape["sp"] == MIDDLE_DILATION and mesh.shape["tp"] == 4
    chosen = local_by_class if split else local
    placed = (
        P(("grp", "sp"), "tp"),
        P(),
        P(None, "tp"),
        P(None, "tp"),
        P(None, "tp"),
        P("tp", None),
        P("tp", None),
        P("tp", None),
    )
    return jax.shard_map(
        chosen,
        mesh=mesh,
        in_specs=placed,
        out_specs=(P(("grp", "sp"), "tp"), P(("grp", "sp"), "tp")),
        check_vma=False,
    )
```

```python
import functools
import math

import jax
import jax.numpy as jnp
import numpy as np
from jax import lax
from jax.experimental import pallas as pl
from jax.experimental.pallas import tpu as pltpu
from jax.sharding import PartitionSpec as P

D = 2048
KEYS_BEHIND = 128
MIDDLE_DILATION = 4
WIDEST_DILATION = 16


EPSILON = 1e-06
ROTARY_BASE = 500000.0


def from_behind(value, axis, steps):
    count = lax.axis_size(axis)
    initial, last = (max(0, -steps), min(count, count - steps))
    return lax.ppermute(value, axis, [(source, source + steps) for source in range(initial, last)])


def rotate(values, positions):
    head_width = values.shape[-1]
    inverse = ROTARY_BASE ** (-jnp.arange(0, head_width, 2, dtype=jnp.float32) / head_width)
    angles = positions[:, None] * inverse[None, :]
    cosine = jnp.cos(angles)[:, None, :]
    sine = jnp.sin(angles)[:, None, :]
    half_width = head_width // 2
    first_half = values[..., :half_width]
    second_half = values[..., half_width:]
    return jnp.concatenate(
        [first_half * cosine - second_half * sine, second_half * cosine + first_half * sine],
        axis=-1,
    )


def head_norm(values, gains):
    normed = values * lax.rsqrt(jnp.mean(values * values, axis=-1, keepdims=True) + EPSILON)
    return normed * gains[None, :, :]


def earlier_pairs(own_pair, token_rows):
    distant_shards = (KEYS_BEHIND * WIDEST_DILATION + token_rows - 1) // token_rows
    pieces = [own_pair]
    for distance in range(1, distant_shards + 1):
        pieces.insert(0, from_behind(own_pair, "sp", distance))
    buffer = jnp.concatenate(pieces, axis=1)
    return buffer


def local_branch(query, key_rows, value_rows, dilation_step, first_pos):
    token_rows, head_count, head_width = query.shape
    reach_rows = KEYS_BEHIND * dilation_step
    buffer_rows = key_rows.shape[0]
    class_rows = token_rows // dilation_step
    class_keys = class_rows + KEYS_BEHIND
    window_start = buffer_rows - token_rows - reach_rows
    key_window = key_rows[window_start:]
    value_window = value_rows[window_start:]
    query_class = query.reshape(class_rows, dilation_step, head_count, head_width).transpose(
        1, 0, 2, 3
    )
    key_class = key_window.reshape(class_keys, dilation_step, head_count, head_width).transpose(
        1, 0, 2, 3
    )
    value_class = value_window.reshape(class_keys, dilation_step, head_count, head_width).transpose(
        1, 0, 2, 3
    )
    block_rows = math.gcd(class_rows, KEYS_BEHIND) if class_rows > KEYS_BEHIND else class_rows
    block_count = class_rows // block_rows
    query_blocks = query_class.reshape(
        dilation_step, block_count, block_rows, head_count, head_width
    )
    key_blocks = jnp.stack(
        [
            key_class[:, number * block_rows : number * block_rows + block_rows + KEYS_BEHIND]
            for number in range(block_count)
        ],
        axis=1,
    )
    value_blocks = jnp.stack(
        [
            value_class[:, number * block_rows : number * block_rows + block_rows + KEYS_BEHIND]
            for number in range(block_count)
        ],
        axis=1,
    )
    scores = jnp.einsum(
        "rnqhd,rnkhd->rnhqk", query_blocks, key_blocks, preferred_element_type=jnp.float32
    ) * head_width ** (-0.5)
    row_index = jnp.arange(block_rows, dtype=jnp.int32)[:, None]
    col_index = jnp.arange(block_rows + KEYS_BEHIND, dtype=jnp.int32)[None, :]
    distance = KEYS_BEHIND + row_index - col_index
    in_band = (distance >= 0) & (distance <= KEYS_BEHIND)
    class_index = jnp.arange(block_count, dtype=jnp.int32)[:, None] * block_rows + col_index
    residue = jnp.arange(dilation_step, dtype=jnp.int32)[:, None, None]
    key_position = first_pos - reach_rows + class_index[None] * dilation_step + residue
    allowed = in_band[None, None, None, :, :] & (key_position >= 0)[:, :, None, None, :]
    scores = jnp.where(allowed, scores, -jnp.inf)
    row_max = jnp.max(scores, axis=-1, keepdims=True)
    weights = jnp.exp(scores - row_max)
    weight_sum = jnp.sum(weights, axis=-1)
    weighted = jnp.einsum(
        "rnhqk,rnkhd->rnqhd",
        weights.astype(jnp.bfloat16),
        value_blocks,
        preferred_element_type=jnp.float32,
    )
    branch_out = weighted / jnp.transpose(weight_sum, (0, 1, 3, 2))[..., None]
    branch_out = branch_out.reshape(dilation_step, class_rows, head_count, head_width).transpose(
        1, 0, 2, 3
    )
    branch_out = branch_out.reshape(token_rows, head_count, head_width)
    log_sum = jnp.transpose(row_max[..., 0] + jnp.log(weight_sum), (0, 1, 3, 2))
    log_sum = (
        log_sum.reshape(dilation_step, class_rows, head_count)
        .transpose(1, 0, 2)
        .reshape(token_rows, head_count)
    )
    return (branch_out, log_sum)


def local(hidden, norm_gain, w_query, w_key, w_value, query_gain, key_gain, w_out):
    token_rows = hidden.shape[0]
    local_width = w_query.shape[1]
    head_count = query_gain.shape[0]
    head_width = query_gain.shape[1]
    gain_full = norm_gain.astype(jnp.float32)
    raw_piece = lax.all_gather(hidden, "tp", axis=1, tiled=True).astype(jnp.float32)
    scaled = (raw_piece * gain_full[None, :]).astype(jnp.bfloat16)

    def add_product(weight):
        return jnp.dot(scaled, weight, preferred_element_type=jnp.float32)

    query_raw = add_product(w_query)
    key_raw = add_product(w_key)
    value_raw = add_product(w_value)
    squares = jnp.sum(raw_piece * raw_piece, axis=1)
    row_scale = lax.rsqrt(squares / D + EPSILON)[:, None]
    first_pos = lax.axis_index("sp") * token_rows
    positions = (jnp.arange(token_rows, dtype=jnp.int32) + first_pos).astype(jnp.float32)
    query = rotate(
        head_norm((query_raw * row_scale).reshape(token_rows, head_count, head_width), query_gain),
        positions,
    ).astype(jnp.bfloat16)
    key_now = rotate(
        head_norm((key_raw * row_scale).reshape(token_rows, head_count, head_width), key_gain),
        positions,
    ).astype(jnp.bfloat16)
    value_now = (value_raw * row_scale).astype(jnp.bfloat16)
    own_pair = jnp.stack([key_now.reshape(token_rows, local_width), value_now], axis=0)
    buffer = earlier_pairs(own_pair, token_rows)
    key_rows = buffer[0].reshape(-1, head_count, head_width)
    value_rows = buffer[1].reshape(-1, head_count, head_width)
    branch_outs = []
    branch_logs = []
    for dilation_step in (1, MIDDLE_DILATION, WIDEST_DILATION):
        branch_out, log_sum = local_branch(query, key_rows, value_rows, dilation_step, first_pos)
        branch_outs.append(branch_out)
        branch_logs.append(log_sum)
    stacked_logs = jnp.stack(branch_logs, axis=0)
    peak = jnp.max(stacked_logs, axis=0)
    log_total = peak + jnp.log(jnp.sum(jnp.exp(stacked_logs - peak[None]), axis=0))
    shares = jnp.exp(stacked_logs - log_total[None])
    attended = jnp.sum(shares[..., None] * jnp.stack(branch_outs, axis=0), axis=0)
    attended = attended.astype(jnp.bfloat16).reshape(token_rows, local_width)
    column_block = lax.all_to_all(w_out, "tp", split_axis=1, concat_axis=0, tiled=True)
    mixed = jnp.dot(
        lax.all_gather(attended, "tp", axis=1, tiled=True),
        column_block,
        preferred_element_type=jnp.float32,
    )
    return (mixed.astype(jnp.bfloat16), log_total)


MESH = pl.DeviceIdType.MESH
LANES = 128


def rotary_table(classes, rows, head_width):
    inverse = (ROTARY_BASE ** (-np.arange(0, head_width, 2, dtype=np.float64) / head_width)).astype(np.float32)
    positions = np.arange(classes * classes * rows, dtype=np.float32)
    angles = (positions[:, None] * inverse[None, :]).astype(np.float64)
    cosine, sine = np.cos(angles), np.sin(angles)
    table = np.concatenate([cosine, cosine, -sine, sine], axis=1).astype(np.float32)
    return table.reshape(classes, rows, classes, 2 * head_width).transpose(0, 2, 1, 3)


def class_kernel(
    hid_ref, gain_ref, qgain_ref, kgain_ref, wq_ref, wk_ref, wv_ref, wo_ref, table_ref,
    mixed_ref, total_ref,
    hb, hc, wall, wo, tb, tc, acc_b, acc_c, q_b, kv_b, kv_c, q_c, halo, oc, lsend, ro, rl, at,
    gain, loc, zs, zr, axs, axr, acs, acr, afs, afr, cxs, cxr, ccs, ccr, cfs, cfr,
    wos, wor, hs, hr, rs, rr, ls, lr, gxs, gxr, gcs, gcr, gfs, gfr,
):
    f32, bf16 = jnp.float32, jnp.bfloat16
    s, p = lax.axis_index("sp"), lax.axis_index("tp")
    n = MIDDLE_DILATION
    rows, width = hid_ref.shape
    sub = rows // n
    heads, hd = qgain_ref.shape
    lw = heads * hd
    halo_sub = halo.shape[1]
    halo_rows = n * halo_sub
    core = p + 1 - 2 * lax.rem(p, 2)
    xp = lax.rem(p + 2, 4)
    diag = lax.rem(core + 2, 4)

    def tp_copy(src, dst, ss, sr, q):
        return pltpu.make_async_remote_copy(
            src_ref=src, dst_ref=dst, send_sem=ss, recv_sem=sr, device_id={"tp": q}, device_id_type=MESH
        )

    def sp_copy(src, dst, ss, sr, q):
        return pltpu.make_async_remote_copy(
            src_ref=src, dst_ref=dst, send_sem=ss, recv_sem=sr, device_id={"sp": q}, device_id_type=MESH
        )

    barrier = pltpu.get_barrier_semaphore()
    for q in (core, xp, diag):
        pl.semaphore_signal(barrier, inc=1, device_id={"tp": q}, device_id_type=MESH)
    for k in range(1, n):
        pl.semaphore_signal(barrier, inc=1, device_id={"sp": lax.rem(s + k, n)}, device_id_type=MESH)
    loads = [
        pltpu.make_async_copy(wq_ref, wall.at[:, pl.ds(0, lw)], loc.at[0]),
        pltpu.make_async_copy(wk_ref, wall.at[:, pl.ds(lw, lw)], loc.at[1]),
        pltpu.make_async_copy(wv_ref, wall.at[:, pl.ds(2 * lw, lw)], loc.at[2]),
        pltpu.make_async_copy(table_ref.at[s], tb, loc.at[3]),
        pltpu.make_async_copy(table_ref.at[:, s], tc, loc.at[4]),
        pltpu.make_async_copy(
            wo_ref.at[:, pl.ds(pl.multiple_of(p * width, LANES), width)], wo.at[p], loc.at[5]
        ),
    ]
    for load in loads:
        load.start()

    def iota(shape, dim):
        return lax.broadcasted_iota(jnp.int32, shape, dim)

    def row_of(r, part):
        return n * lax.rem(r, part) + r // part

    square = (rows, rows)
    to_class = (row_of(iota(square, 0), sub) == iota(square, 1)).astype(f32).astype(bf16)
    flat_gain = gain_ref[...].astype(f32)
    for j in range(flat_gain.shape[0]):
        each = width // LANES
        gain[j // each, :, (j % each) * LANES : (j % each + 1) * LANES] = flat_gain[j : j + 1]
    permuted = jnp.dot(to_class, hid_ref[...], preferred_element_type=f32).astype(bf16)
    hb[p] = permuted.reshape(n, sub, width)
    hc[p, s] = hb[p, s]
    pl.semaphore_wait(barrier, 3 + n - 1)

    sends = []

    def go(copy):
        copy.start()
        sends.append(copy)
        return copy

    za = [None] + [
        go(sp_copy(hb.at[p, lax.rem(s + k, n)], hc.at[p, s], zs.at[k], zr.at[k], lax.rem(s + k, n)))
        for k in range(1, n)
    ]
    ax = [go(tp_copy(hb.at[p, i], hb.at[p, i], axs.at[i], axr.at[i], xp)) for i in range(n)]
    ac = go(tp_copy(hb.at[p], hb.at[p], acs, acr, core))

    block_of = [lax.rem(s + n - k, n) for k in range(n)]
    cx, cc = [], []

    def spread(k):
        piece = hc.at[p, block_of[k]]
        cx.append(go(tp_copy(piece, piece, cxs.at[k], cxr.at[k], xp)))
        cc.append(go(tp_copy(piece, piece, ccs.at[k], ccr.at[k], core)))

    spread(0)

    def chunk(source, q):
        raw = source[q].reshape(rows, width).astype(f32)
        scaled = (raw * gain[q]).astype(bf16)
        w = wall[pl.ds(pl.multiple_of(q * width, LANES), width), :]
        return jnp.dot(scaled, w, preferred_element_type=f32), jnp.sum(raw * raw, axis=1, keepdims=True)

    for load in loads:
        load.wait()
    acc_b[...], sq_b = chunk(hb, p)
    ac.wait_recv()
    prod, more = chunk(hb, core)
    acc_b[...] += prod
    sq_b += more

    af = []
    for i in range(n):
        ax[i].wait_recv()
        af.append(go(tp_copy(hb.at[xp, i], hb.at[xp, i], afs.at[i], afr.at[i], core)))
        if i >= 1:
            za[i].wait_recv()
            spread(i)
    w_sends = []
    for j, q in enumerate((core, xp, diag)):
        w_sends.append(
            go(tp_copy(wo_ref.at[:, pl.ds(pl.multiple_of(q * width, LANES), width)], wo.at[p], wos.at[j], wor.at[j], q))
        )

    prod, more = chunk(hb, xp)
    acc_b[...] += prod
    sq_b += more
    for copy in af:
        copy.wait_recv()
    prod, more = chunk(hb, diag)
    sq_b += more

    def finish(acc, sq, table, q_out, kv_out):
        raw = acc * lax.rsqrt(sq / (width * 4) + EPSILON)
        table = table[...].reshape(rows, 2 * hd)
        cosine, sine = table[:, :hd], table[:, hd:]
        for h in range(heads):
            for start, gains, out in ((0, qgain_ref, q_out), (lw, kgain_ref, kv_out)):
                x = raw[:, start + h * hd : start + (h + 1) * hd]
                x = x * lax.rsqrt(jnp.mean(x * x, axis=-1, keepdims=True) + EPSILON)
                x = x * gains[pl.ds(h, 1), :]
                x = x * cosine + pltpu.roll(x, hd // 2, 1) * sine
                out[:, :, h * hd : (h + 1) * hd] = x.astype(bf16).reshape(n, sub, hd)
        kv_out[:, :, lw:] = raw[:, 2 * lw :].astype(bf16).reshape(n, sub, lw)

    finish(acc_b[...] + prod, sq_b, tb, q_b, kv_b)
    halo_send = sp_copy(kv_b.at[:, pl.ds(sub - halo_sub, halo_sub), :], halo, hs, hr, lax.rem(s + 1, n))

    @pl.when(s < n - 1)
    def _():
        halo_send.start()

    @pl.when(s == 0)
    def _():
        halo[...] = jnp.zeros_like(halo)

    cf = []
    for k in range(n):
        cx[k].wait_recv()
        piece = hc.at[xp, block_of[k]]
        cf.append(go(tp_copy(piece, piece, cfs.at[k], cfr.at[k], core)))
        if k == n - 2:
            for copy in cc:
                copy.wait_recv()
            prod, sq_c = chunk(hc, p)
            prod2, more = chunk(hc, core)
            acc_c[...] = prod + prod2
            sq_c += more
    prod, more = chunk(hc, xp)
    acc_c[...] += prod
    sq_c += more
    for copy in cf:
        copy.wait_recv()
    prod, more = chunk(hc, diag)
    sq_c += more
    finish(acc_c[...] + prod, sq_c, tc, q_c, kv_c)

    def attend(q, k, v, bias):
        score = lax.dot_general(q, k, (((1,), (1,)), ((), ())), preferred_element_type=f32)
        score = score * hd ** (-0.5) + bias
        top = jnp.max(score, axis=-1, keepdims=True)
        weight = jnp.exp(score - top)
        total = jnp.sum(weight, axis=-1, keepdims=True)
        out = jnp.dot(weight.astype(bf16), v, preferred_element_type=f32) / total
        return out, top + jnp.log(total)

    behind = iota(square, 0) - iota(square, 1)
    stride = WIDEST_DILATION // n
    near = (behind >= 0) & (behind <= KEYS_BEHIND)
    far = (behind >= 0) & (behind <= KEYS_BEHIND * stride) & ((behind + rows * stride) % stride == 0)
    bias_c = jnp.where(
        near & far, math.log(2.0), jnp.where(near | far, 0.0, -jnp.inf)
    ).astype(f32)
    lane = iota((rows, LANES), 1)
    logs = jnp.zeros((rows, LANES), f32)
    for h in range(heads):
        cols = slice(h * hd, (h + 1) * hd)
        vcols = slice(lw + h * hd, lw + (h + 1) * hd)
        out, lse = attend(
            q_c[:, :, cols].reshape(rows, hd), kv_c[:, :, cols].reshape(rows, hd),
            kv_c[:, :, vcols].reshape(rows, hd), bias_c,
        )
        oc[:, :, cols] = out.astype(bf16).reshape(n, sub, hd)
        logs = jnp.where(lane == h, lse, logs)
    pad = LANES - sub
    for b in range(n):
        part = jnp.concatenate([logs[b * sub : (b + 1) * sub], jnp.zeros((pad, LANES), f32)], axis=0)
        lsend[b] = jnp.transpose(part)[:8]
    back, back_l = [], []
    for k in range(1, n):
        to = lax.rem(s + k, n)
        back.append(go(sp_copy(oc.at[to], ro.at[s], rs.at[k], rr.at[k], to)))
        back_l.append(go(sp_copy(lsend.at[to], rl.at[s], ls.at[k], lr.at[k], to)))
    ro[s] = oc[s]
    rl[s] = lsend[s]

    @pl.when(s > 0)
    def _():
        halo_send.wait_recv()

    total_keys = rows + halo_rows
    wide = (rows, total_keys)
    key = iota(wide, 1)
    key_row = jnp.where(key < rows, row_of(key, sub), row_of(key - rows, halo_sub) - halo_rows)
    behind = row_of(iota(wide, 0), sub) - key_row
    ok = (behind >= 0) & (behind <= KEYS_BEHIND) & (key_row + s * rows >= 0)
    bias_b = jnp.where(ok, 0.0, -jnp.inf).astype(f32)
    near_parts = []
    for h in range(heads):
        cols = slice(h * hd, (h + 1) * hd)
        vcols = slice(lw + h * hd, lw + (h + 1) * hd)
        near_parts.append(attend(
            q_b[:, :, cols].reshape(rows, hd),
            jnp.concatenate([kv_b[:, :, cols].reshape(rows, hd), halo[:, :, cols].reshape(halo_rows, hd)], axis=0),
            jnp.concatenate([kv_b[:, :, vcols].reshape(rows, hd), halo[:, :, vcols].reshape(halo_rows, hd)], axis=0),
            bias_b,
        ))

    for copy in back + back_l:
        copy.wait_recv()
    far_logs = jnp.concatenate(
        [
            jnp.transpose(jnp.concatenate([rl[i], jnp.zeros((LANES - 8, LANES), f32)], axis=0))[:sub]
            for i in range(n)
        ],
        axis=0,
    )
    logs = jnp.zeros((rows, LANES), f32)
    mixed_heads = []
    for h in range(heads):
        out, lse = near_parts[h]
        far_lse = far_logs[:, h : h + 1]
        far_out = ro[:, :, h * hd : (h + 1) * hd].reshape(rows, hd).astype(f32)
        top = jnp.maximum(lse, far_lse)
        e_near, e_far = jnp.exp(lse - top), jnp.exp(far_lse - top)
        both = e_near + e_far
        logs = jnp.where(lane == h, top + jnp.log(both), logs)
        mixed_heads.append(((e_near * out + e_far * far_out) / both).astype(bf16))
    attended = jnp.concatenate(mixed_heads, axis=1)
    from_class = (iota(square, 0) == row_of(iota(square, 1), sub)).astype(f32).astype(bf16)
    at[p] = jnp.dot(from_class, attended, preferred_element_type=f32).astype(bf16)
    half = rows // 2
    gx = [
        go(tp_copy(at.at[p, pl.ds(i * half, half)], at.at[p, pl.ds(i * half, half)], gxs.at[i], gxr.at[i], xp))
        for i in range(2)
    ]
    gc = go(tp_copy(at.at[p], at.at[p], gcs, gcr, core))
    high = logs.astype(bf16)
    rest = logs - high.astype(f32)
    middle = rest.astype(bf16)
    low = (rest - middle.astype(f32)).astype(bf16)
    ordered = sum(jnp.dot(from_class, x, preferred_element_type=f32) for x in (high, middle, low))
    for j in range(rows // LANES):
        block = slice(j * LANES, (j + 1) * LANES)
        total_ref[:, block] = jnp.transpose(ordered[block])[:heads]

    result = jnp.dot(at[p], wo[p], preferred_element_type=f32)
    for copy in w_sends:
        copy.wait_recv()
    gc.wait_recv()
    result += jnp.dot(at[core], wo[core], preferred_element_type=f32)
    gf = []
    for i in range(2):
        gx[i].wait_recv()
        piece = at.at[xp, pl.ds(i * half, half)]
        gf.append(go(tp_copy(piece, piece, gfs.at[i], gfr.at[i], core)))
    result += jnp.dot(at[xp], wo[xp], preferred_element_type=f32)
    for copy in gf:
        copy.wait_recv()
    result += jnp.dot(at[diag], wo[diag], preferred_element_type=f32)
    mixed_ref[...] = result.astype(bf16)
    for copy in sends:
        copy.wait_send()

    @pl.when(s < n - 1)
    def _():
        halo_send.wait_send()


def local_by_class(hidden, norm_gain, w_query, w_key, w_value, query_gain, key_gain, w_out):
    n = MIDDLE_DILATION
    rows, width = hidden.shape
    heads, hd = query_gain.shape
    lw = heads * hd
    sub = rows // n
    halo_sub = KEYS_BEHIND // n
    bf16, f32 = jnp.bfloat16, jnp.float32
    table = jnp.asarray(rotary_table(n, sub, hd))
    vmem = pl.BlockSpec(memory_space=pltpu.VMEM)
    anyspace = pl.BlockSpec(memory_space=pl.ANY)
    dma = pltpu.SemaphoreType.DMA
    mixed, total = pl.pallas_call(
        class_kernel,
        out_shape=(
            pltpu.VMEM((rows, w_out.shape[1] // 4), bf16),
            pltpu.VMEM((heads, rows), f32),
        ),
        in_specs=[vmem] * 4 + [anyspace] * 5,
        out_specs=(vmem, vmem),
        scratch_shapes=[
            pltpu.VMEM((4, n, sub, width), bf16),
            pltpu.VMEM((4, n, sub, width), bf16),
            pltpu.VMEM((4 * width, 3 * lw), bf16),
            pltpu.VMEM((4, lw, width), bf16),
            pltpu.VMEM((n, sub, 2 * hd), f32),
            pltpu.VMEM((n, sub, 2 * hd), f32),
            pltpu.VMEM((rows, 3 * lw), f32),
            pltpu.VMEM((rows, 3 * lw), f32),
            pltpu.VMEM((n, sub, lw), bf16),
            pltpu.VMEM((n, sub, 2 * lw), bf16),
            pltpu.VMEM((n, sub, 2 * lw), bf16),
            pltpu.VMEM((n, sub, lw), bf16),
            pltpu.VMEM((n, halo_sub, 2 * lw), bf16),
            pltpu.VMEM((n, sub, lw), bf16),
            pltpu.VMEM((n, 8, LANES), f32),
            pltpu.VMEM((n, sub, lw), bf16),
            pltpu.VMEM((n, 8, LANES), f32),
            pltpu.VMEM((4, rows, lw), bf16),
            pltpu.VMEM((4, 1, width), f32),
            dma((6,)),
            dma((n,)), dma((n,)),
            dma((n,)), dma((n,)), dma, dma, dma((n,)), dma((n,)),
            dma((n,)), dma((n,)), dma((n,)), dma((n,)), dma((n,)), dma((n,)),
            dma((3,)), dma((3,)),
            dma, dma,
            dma((n,)), dma((n,)), dma((n,)), dma((n,)),
            dma((2,)), dma((2,)), dma, dma, dma((2,)), dma((2,)),
        ],
        compiler_params=pltpu.CompilerParams(
            collective_id=0, has_side_effects=True, vmem_limit_bytes=60 * 1024 * 1024
        ),
    )(
        hidden, norm_gain.reshape(-1, LANES), query_gain, key_gain,
        w_query, w_key, w_value, w_out, table,
    )
    return mixed, total.T


def solution(mesh):
    split = mesh.shape["sp"] == MIDDLE_DILATION and mesh.shape["tp"] == 4
    chosen = local_by_class if split else local
    placed = (
        P(("grp", "sp"), "tp"),
        P(),
        P(None, "tp"),
        P(None, "tp"),
        P(None, "tp"),
        P("tp", None),
        P("tp", None),
        P("tp", None),
    )
    return jax.shard_map(
        chosen,
        mesh=mesh,
        in_specs=placed,
        out_specs=(P(("grp", "sp"), "tp"), P(("grp", "sp"), "tp")),
        check_vma=False,
    )
```

```python
import functools
import math

import jax
import jax.numpy as jnp
import numpy as np
from jax import lax
from jax.experimental import pallas as pl
from jax.experimental.pallas import tpu as pltpu
from jax.sharding import PartitionSpec as P

D = 2048
KEYS_BEHIND = 128
MIDDLE_DILATION = 4
WIDEST_DILATION = 16


EPSILON = 1e-06
ROTARY_BASE = 500000.0


def from_behind(value, axis, steps):
    count = lax.axis_size(axis)
    initial, last = (max(0, -steps), min(count, count - steps))
    return lax.ppermute(value, axis, [(source, source + steps) for source in range(initial, last)])


def rotate(values, positions):
    head_width = values.shape[-1]
    inverse = ROTARY_BASE ** (-jnp.arange(0, head_width, 2, dtype=jnp.float32) / head_width)
    angles = positions[:, None] * inverse[None, :]
    cosine = jnp.cos(angles)[:, None, :]
    sine = jnp.sin(angles)[:, None, :]
    half_width = head_width // 2
    first_half = values[..., :half_width]
    second_half = values[..., half_width:]
    return jnp.concatenate(
        [first_half * cosine - second_half * sine, second_half * cosine + first_half * sine],
        axis=-1,
    )


def head_norm(values, gains):
    normed = values * lax.rsqrt(jnp.mean(values * values, axis=-1, keepdims=True) + EPSILON)
    return normed * gains[None, :, :]


def earlier_pairs(own_pair, token_rows):
    distant_shards = (KEYS_BEHIND * WIDEST_DILATION + token_rows - 1) // token_rows
    pieces = [own_pair]
    for distance in range(1, distant_shards + 1):
        pieces.insert(0, from_behind(own_pair, "sp", distance))
    buffer = jnp.concatenate(pieces, axis=1)
    return buffer


def local_branch(query, key_rows, value_rows, dilation_step, first_pos):
    token_rows, head_count, head_width = query.shape
    reach_rows = KEYS_BEHIND * dilation_step
    buffer_rows = key_rows.shape[0]
    class_rows = token_rows // dilation_step
    class_keys = class_rows + KEYS_BEHIND
    window_start = buffer_rows - token_rows - reach_rows
    key_window = key_rows[window_start:]
    value_window = value_rows[window_start:]
    query_class = query.reshape(class_rows, dilation_step, head_count, head_width).transpose(
        1, 0, 2, 3
    )
    key_class = key_window.reshape(class_keys, dilation_step, head_count, head_width).transpose(
        1, 0, 2, 3
    )
    value_class = value_window.reshape(class_keys, dilation_step, head_count, head_width).transpose(
        1, 0, 2, 3
    )
    block_rows = math.gcd(class_rows, KEYS_BEHIND) if class_rows > KEYS_BEHIND else class_rows
    block_count = class_rows // block_rows
    query_blocks = query_class.reshape(
        dilation_step, block_count, block_rows, head_count, head_width
    )
    key_blocks = jnp.stack(
        [
            key_class[:, number * block_rows : number * block_rows + block_rows + KEYS_BEHIND]
            for number in range(block_count)
        ],
        axis=1,
    )
    value_blocks = jnp.stack(
        [
            value_class[:, number * block_rows : number * block_rows + block_rows + KEYS_BEHIND]
            for number in range(block_count)
        ],
        axis=1,
    )
    scores = jnp.einsum(
        "rnqhd,rnkhd->rnhqk", query_blocks, key_blocks, preferred_element_type=jnp.float32
    ) * head_width ** (-0.5)
    row_index = jnp.arange(block_rows, dtype=jnp.int32)[:, None]
    col_index = jnp.arange(block_rows + KEYS_BEHIND, dtype=jnp.int32)[None, :]
    distance = KEYS_BEHIND + row_index - col_index
    in_band = (distance >= 0) & (distance <= KEYS_BEHIND)
    class_index = jnp.arange(block_count, dtype=jnp.int32)[:, None] * block_rows + col_index
    residue = jnp.arange(dilation_step, dtype=jnp.int32)[:, None, None]
    key_position = first_pos - reach_rows + class_index[None] * dilation_step + residue
    allowed = in_band[None, None, None, :, :] & (key_position >= 0)[:, :, None, None, :]
    scores = jnp.where(allowed, scores, -jnp.inf)
    row_max = jnp.max(scores, axis=-1, keepdims=True)
    weights = jnp.exp(scores - row_max)
    weight_sum = jnp.sum(weights, axis=-1)
    weighted = jnp.einsum(
        "rnhqk,rnkhd->rnqhd",
        weights.astype(jnp.bfloat16),
        value_blocks,
        preferred_element_type=jnp.float32,
    )
    branch_out = weighted / jnp.transpose(weight_sum, (0, 1, 3, 2))[..., None]
    branch_out = branch_out.reshape(dilation_step, class_rows, head_count, head_width).transpose(
        1, 0, 2, 3
    )
    branch_out = branch_out.reshape(token_rows, head_count, head_width)
    log_sum = jnp.transpose(row_max[..., 0] + jnp.log(weight_sum), (0, 1, 3, 2))
    log_sum = (
        log_sum.reshape(dilation_step, class_rows, head_count)
        .transpose(1, 0, 2)
        .reshape(token_rows, head_count)
    )
    return (branch_out, log_sum)


def local(hidden, norm_gain, w_query, w_key, w_value, query_gain, key_gain, w_out):
    token_rows = hidden.shape[0]
    local_width = w_query.shape[1]
    head_count = query_gain.shape[0]
    head_width = query_gain.shape[1]
    gain_full = norm_gain.astype(jnp.float32)
    raw_piece = lax.all_gather(hidden, "tp", axis=1, tiled=True).astype(jnp.float32)
    scaled = (raw_piece * gain_full[None, :]).astype(jnp.bfloat16)

    def add_product(weight):
        return jnp.dot(scaled, weight, preferred_element_type=jnp.float32)

    query_raw = add_product(w_query)
    key_raw = add_product(w_key)
    value_raw = add_product(w_value)
    squares = jnp.sum(raw_piece * raw_piece, axis=1)
    row_scale = lax.rsqrt(squares / D + EPSILON)[:, None]
    first_pos = lax.axis_index("sp") * token_rows
    positions = (jnp.arange(token_rows, dtype=jnp.int32) + first_pos).astype(jnp.float32)
    query = rotate(
        head_norm((query_raw * row_scale).reshape(token_rows, head_count, head_width), query_gain),
        positions,
    ).astype(jnp.bfloat16)
    key_now = rotate(
        head_norm((key_raw * row_scale).reshape(token_rows, head_count, head_width), key_gain),
        positions,
    ).astype(jnp.bfloat16)
    value_now = (value_raw * row_scale).astype(jnp.bfloat16)
    own_pair = jnp.stack([key_now.reshape(token_rows, local_width), value_now], axis=0)
    buffer = earlier_pairs(own_pair, token_rows)
    key_rows = buffer[0].reshape(-1, head_count, head_width)
    value_rows = buffer[1].reshape(-1, head_count, head_width)
    branch_outs = []
    branch_logs = []
    for dilation_step in (1, MIDDLE_DILATION, WIDEST_DILATION):
        branch_out, log_sum = local_branch(query, key_rows, value_rows, dilation_step, first_pos)
        branch_outs.append(branch_out)
        branch_logs.append(log_sum)
    stacked_logs = jnp.stack(branch_logs, axis=0)
    peak = jnp.max(stacked_logs, axis=0)
    log_total = peak + jnp.log(jnp.sum(jnp.exp(stacked_logs - peak[None]), axis=0))
    shares = jnp.exp(stacked_logs - log_total[None])
    attended = jnp.sum(shares[..., None] * jnp.stack(branch_outs, axis=0), axis=0)
    attended = attended.astype(jnp.bfloat16).reshape(token_rows, local_width)
    column_block = lax.all_to_all(w_out, "tp", split_axis=1, concat_axis=0, tiled=True)
    mixed = jnp.dot(
        lax.all_gather(attended, "tp", axis=1, tiled=True),
        column_block,
        preferred_element_type=jnp.float32,
    )
    return (mixed.astype(jnp.bfloat16), log_total)


MESH = pl.DeviceIdType.MESH
LANES = 128


def rotary_table(classes, rows, head_width):
    inverse = (ROTARY_BASE ** (-np.arange(0, head_width, 2, dtype=np.float64) / head_width)).astype(np.float32)
    positions = np.arange(classes * classes * rows, dtype=np.float32)
    angles = (positions[:, None] * inverse[None, :]).astype(np.float64)
    cosine, sine = np.cos(angles), np.sin(angles)
    table = np.concatenate([cosine, cosine, -sine, sine], axis=1).astype(np.float32)
    return table.reshape(classes, rows, classes, 2 * head_width).transpose(0, 2, 1, 3)


def class_kernel(
    hid_ref, gain_ref, qgain_ref, kgain_ref, wq_ref, wk_ref, wv_ref, wo_ref, table_ref,
    mixed_ref, total_ref,
    hid, gain_in, qgain, kgain, hb, hc, wall, wo, tb, tc, acc_b, acc_c, q_b, kv_b, kv_c, q_c,
    halo, oc, lsend, ro, rl, near_out, near_log, all_log, at, gain,
    loc, zs, zr, axs, axr, acs, acr, afs, afr, cxs, cxr, ccs, ccr, cfs, cfr,
    wos, wor, wfs, wfr, hs, hr, rs, rr, ls, lr, gxs, gxr, gcs, gcr, gfs, gfr,
):
    f32, bf16 = jnp.float32, jnp.bfloat16
    g, s, p = lax.axis_index("grp"), lax.axis_index("sp"), lax.axis_index("tp")
    n = MIDDLE_DILATION
    rows, width = hid_ref.shape
    sub = rows // n
    heads, hd = qgain_ref.shape
    lw = heads * hd
    halo_sub = halo.shape[1]
    halo_rows = n * halo_sub
    core = p + 1 - 2 * lax.rem(p, 2)
    xp = lax.rem(p + 2, 4)
    diag = lax.rem(core + 2, 4)
    order = (1, 3, 2)

    def copy_to(axis, src, dst, ss, sr, q):
        return pltpu.make_async_remote_copy(
            src_ref=src, dst_ref=dst, send_sem=ss, recv_sem=sr, device_id={axis: q}, device_id_type=MESH
        )

    tp_copy = functools.partial(copy_to, "tp")
    sp_copy = functools.partial(copy_to, "sp")
    load_hid = pltpu.make_async_copy(hid_ref, hid, loc.at[6])
    load_hid.start()
    barrier = pltpu.get_barrier_semaphore()
    for q in (core, xp, diag):
        pl.semaphore_signal(barrier, inc=1, device_id={"tp": q}, device_id_type=MESH)
    for k in range(1, n):
        pl.semaphore_signal(barrier, inc=1, device_id={"sp": lax.rem(s + k, n)}, device_id_type=MESH)
    pl.semaphore_signal(barrier, inc=1, device_id={"grp": 1 - g}, device_id_type=MESH)
    loads = [
        pltpu.make_async_copy(gain_ref, gain_in, loc.at[7]),
        pltpu.make_async_copy(qgain_ref, qgain, loc.at[8]),
        pltpu.make_async_copy(kgain_ref, kgain, loc.at[9]),
        pltpu.make_async_copy(wq_ref, wall.at[:, pl.ds(0, lw)], loc.at[0]),
        pltpu.make_async_copy(wk_ref, wall.at[:, pl.ds(lw, lw)], loc.at[1]),
        pltpu.make_async_copy(wv_ref, wall.at[:, pl.ds(2 * lw, lw)], loc.at[2]),
        pltpu.make_async_copy(table_ref.at[s], tb, loc.at[3]),
        pltpu.make_async_copy(table_ref.at[:, s], tc, loc.at[4]),
        pltpu.make_async_copy(
            wo_ref.at[:, pl.ds(pl.multiple_of(p * width, LANES), width)], wo.at[p], loc.at[5]
        ),
    ]
    for load in loads:
        load.start()

    def iota(shape, dim):
        return lax.broadcasted_iota(jnp.int32, shape, dim)

    def row_of(r, part):
        return n * lax.rem(r, part) + r // part

    square = (rows, rows)
    to_class = (row_of(iota(square, 0), sub) == iota(square, 1)).astype(f32).astype(bf16)
    load_hid.wait()
    permuted = jnp.dot(to_class, hid[...], preferred_element_type=f32).astype(bf16)
    hb[p] = permuted.reshape(n, sub, width)
    pl.semaphore_wait(barrier, 3 + n)

    sends = []

    def go(copy):
        copy.start()
        sends.append(copy)
        return copy

    za = {}
    for k in order:
        to = lax.rem(s + k, n)
        za[k] = go(sp_copy(hb.at[p, to], hc.at[p, s], zs.at[k], zr.at[k], to))
    ax = [go(tp_copy(hb.at[p, i], hb.at[p, i], axs.at[i], axr.at[i], xp)) for i in range(n)]
    ac = go(tp_copy(hb.at[p], hb.at[p], acs, acr, core))

    block_of = [lax.rem(s + n - k, n) for k in range(n)]
    cx, cc, cf = {}, {}, {}

    def spread(k):
        piece = hc.at[p, block_of[k]]
        cx[k] = go(tp_copy(piece, piece, cxs.at[k], cxr.at[k], xp))
        cc[k] = go(tp_copy(piece, piece, ccs.at[k], ccr.at[k], core))

    for load in loads:
        load.wait()
    flat_gain = gain_in[...].astype(f32)
    for j in range(flat_gain.shape[0]):
        each = width // LANES
        gain[j // each, :, (j % each) * LANES : (j % each + 1) * LANES] = flat_gain[j : j + 1]

    def chunk(raw, q):
        raw = raw.astype(f32)
        scaled = (raw * gain[q]).astype(bf16)
        w = wall[pl.ds(pl.multiple_of(q * width, LANES), width), :]
        return jnp.dot(scaled, w, preferred_element_type=f32), jnp.sum(raw * raw, axis=1, keepdims=True)

    def chunk_b(q):
        return chunk(hb[q].reshape(rows, width), q)

    def chunk_c(k, q):
        return chunk(hb[q, s] if k == 0 else hc[q, block_of[k]], q)

    acc_b[...], sq_b = chunk_b(p)
    ac.wait_recv()
    prod, more = chunk_b(core)
    acc_b[...] += prod
    sq_b += more

    af = []
    for i in range(n):
        ax[i].wait_recv()
        af.append(go(tp_copy(hb.at[xp, i], hb.at[xp, i], afs.at[i], afr.at[i], core)))
        if i >= 1:
            za[order[i - 1]].wait_recv()
            spread(order[i - 1])
    half = lw // 2
    mine = pl.ds(pl.multiple_of(g * half, 8), half)
    w_sends = [
        go(tp_copy(wo_ref.at[:, pl.ds(pl.multiple_of(core * width, LANES), width)], wo.at[p], wos.at[0], wor.at[0], core))
    ]
    for j, q in ((1, xp), (2, diag)):
        w_sends.append(go(tp_copy(
            wo_ref.at[mine, pl.ds(pl.multiple_of(q * width, LANES), width)], wo.at[p, mine], wos.at[j], wor.at[j], q
        )))

    prod, more = chunk_b(xp)
    acc_b[...] += prod
    sq_b += more
    for copy in af:
        copy.wait_recv()
    prod, more = chunk_b(diag)
    sq_b += more

    def finish(acc, sq, table, put_q, put_kv):
        raw = acc * lax.rsqrt(sq / (width * 4) + EPSILON)
        cosine, sine = table[:, :hd], table[:, hd:]
        for h in range(heads):
            for start, gains, put in ((0, qgain, put_q), (lw, kgain, put_kv)):
                x = raw[:, start + h * hd : start + (h + 1) * hd]
                x = x * lax.rsqrt(jnp.mean(x * x, axis=-1, keepdims=True) + EPSILON)
                x = x * gains[pl.ds(h, 1), :]
                x = x * cosine + pltpu.roll(x, hd // 2, 1) * sine
                put(slice(h * hd, (h + 1) * hd), x.astype(bf16))
        put_kv(slice(lw, 2 * lw), raw[:, 2 * lw :].astype(bf16))

    def put_all(ref):
        def put(cols, x):
            ref[:, :, cols] = x.reshape(n, sub, x.shape[1])
        return put

    def put_block(ref, b):
        def put(cols, x):
            ref[b, :, cols] = x
        return put

    finish(acc_b[...] + prod, sq_b, tb[...].reshape(rows, 2 * hd), put_all(q_b), put_all(kv_b))
    halo_send = sp_copy(kv_b.at[:, pl.ds(sub - halo_sub, halo_sub), :], halo, hs, hr, lax.rem(s + 1, n))

    @pl.when(s < n - 1)
    def _():
        halo_send.start()

    @pl.when(s == 0)
    def _():
        halo[...] = jnp.zeros_like(halo)

    def finish_c(k, acc, sq):
        prod, more = chunk_c(k, diag)
        b = block_of[k]
        finish(acc + prod, sq + more, tc[b], put_block(q_c, b), put_block(kv_c, b))

    acc_0, sq_0 = chunk_c(0, p)
    for q in (core, xp):
        prod, more = chunk_c(0, q)
        acc_0 += prod
        sq_0 += more
    finish_c(0, acc_0, sq_0)
    before, squares = None, {}
    for k in order:
        cc[k].wait_recv()
        part, squares[k] = chunk_c(k, p)
        prod, more = chunk_c(k, core)
        part += prod
        squares[k] += more
        cx[k].wait_recv()
        piece = hc.at[xp, block_of[k]]
        cf[k] = go(tp_copy(piece, piece, cfs.at[k], cfr.at[k], core))
        prod, more = chunk_c(k, xp)
        squares[k] += more
        acc_c[k] = part + prod
        if before is not None:
            cf[before].wait_recv()
            finish_c(before, acc_c[before], squares[before])
        before = k
    cf[before].wait_recv()
    finish_c(before, acc_c[before], squares[before])

    def attend(q, k, v, bias):
        score = lax.dot_general(q, k, (((1,), (1,)), ((), ())), preferred_element_type=f32)
        score = score * hd ** (-0.5) + bias
        top = jnp.max(score, axis=-1, keepdims=True)
        weight = jnp.exp(score - top)
        total = jnp.sum(weight, axis=-1, keepdims=True)
        out = jnp.dot(weight.astype(bf16), v, preferred_element_type=f32) / total
        return out, top + jnp.log(total)

    behind = iota(square, 0) - iota(square, 1)
    stride = WIDEST_DILATION // n
    near = (behind >= 0) & (behind <= KEYS_BEHIND)
    far = (behind >= 0) & (behind <= KEYS_BEHIND * stride) & ((behind + rows * stride) % stride == 0)
    bias_c = jnp.where(
        near & far, math.log(2.0), jnp.where(near | far, 0.0, -jnp.inf)
    ).astype(f32)
    lane = iota((rows, LANES), 1)
    logs = jnp.zeros((rows, LANES), f32)
    back = {k: [] for k in order}
    for h in range(heads):
        cols = slice(h * hd, (h + 1) * hd)
        vcols = slice(lw + h * hd, lw + (h + 1) * hd)
        out, lse = attend(
            q_c[:, :, cols].reshape(rows, hd), kv_c[:, :, cols].reshape(rows, hd),
            kv_c[:, :, vcols].reshape(rows, hd), bias_c,
        )
        oc[h] = out.astype(bf16).reshape(n, sub, hd)
        logs = jnp.where(lane == h, lse, logs)
        for k in order:
            to = lax.rem(s + k, n)
            back[k].append(go(sp_copy(oc.at[h, to], ro.at[h, s], rs.at[h, k], rr.at[h, k], to)))
    pad = LANES - sub
    for b in range(n):
        part = jnp.concatenate([logs[b * sub : (b + 1) * sub], jnp.zeros((pad, LANES), f32)], axis=0)
        lsend[b] = jnp.transpose(part)[:8]
    for k in order:
        to = lax.rem(s + k, n)
        back[k].append(go(sp_copy(lsend.at[to], rl.at[s], ls.at[k], lr.at[k], to)))

    @pl.when(s > 0)
    def _():
        halo_send.wait_recv()

    total_keys = rows + halo_rows
    wide = (rows, total_keys)
    key = iota(wide, 1)
    key_row = jnp.where(key < rows, row_of(key, sub), row_of(key - rows, halo_sub) - halo_rows)
    behind = row_of(iota(wide, 0), sub) - key_row
    ok = (behind >= 0) & (behind <= KEYS_BEHIND) & (key_row + s * rows >= 0)
    bias_b = jnp.where(ok, 0.0, -jnp.inf).astype(f32)
    logs = jnp.zeros((rows, LANES), f32)
    for h in range(heads):
        cols = slice(h * hd, (h + 1) * hd)
        vcols = slice(lw + h * hd, lw + (h + 1) * hd)
        out, lse = attend(
            q_b[:, :, cols].reshape(rows, hd),
            jnp.concatenate([kv_b[:, :, cols].reshape(rows, hd), halo[:, :, cols].reshape(halo_rows, hd)], axis=0),
            jnp.concatenate([kv_b[:, :, vcols].reshape(rows, hd), halo[:, :, vcols].reshape(halo_rows, hd)], axis=0),
            bias_b,
        )
        near_out[h] = out.reshape(n, sub, hd)
        logs = jnp.where(lane == h, lse, logs)
    near_log[...] = logs.reshape(n, sub, LANES)

    wf = []
    for j, q in ((1, xp), (2, diag)):
        w_sends[j].wait_recv()
        wf.append(go(copy_to("grp", wo.at[q, mine], wo.at[q, mine], wfs.at[j - 1], wfr.at[j - 1], 1 - g)))

    gx, gc, gf = {}, {}, {}

    def merge(k):
        b = block_of[k]
        received = lsend[s] if k == 0 else rl[b]
        far_log = jnp.transpose(jnp.concatenate([received, jnp.zeros((LANES - 8, LANES), f32)], axis=0))[:sub]
        logs = jnp.zeros((sub, LANES), f32)
        for h in range(heads):
            lse = near_log[b][:, h : h + 1]
            far_lse = far_log[:, h : h + 1]
            far_out = (oc[h, s] if k == 0 else ro[h, b]).astype(f32)
            top = jnp.maximum(lse, far_lse)
            e_near, e_far = jnp.exp(lse - top), jnp.exp(far_lse - top)
            both = e_near + e_far
            logs = jnp.where(lane[:sub] == h, top + jnp.log(both), logs)
            at[p, b, :, h * hd : (h + 1) * hd] = ((e_near * near_out[h, b] + e_far * far_out) / both).astype(bf16)
        all_log[b] = logs
        piece = at.at[p, b]
        gx[k] = go(tp_copy(piece, piece, gxs.at[k], gxr.at[k], xp))
        gc[k] = go(tp_copy(piece, piece, gcs.at[k], gcr.at[k], core))

    def forward(k):
        gx[k].wait_recv()
        piece = at.at[xp, block_of[k]]
        gf[k] = go(tp_copy(piece, piece, gfs.at[k], gfr.at[k], core))

    merge(0)
    for k, ready in zip(order, (None, 0, order[0])):
        for copy in back[k]:
            copy.wait_recv()
        merge(k)
        if ready is not None:
            forward(ready)
    from_class = (iota(square, 0) == row_of(iota(square, 1), sub)).astype(f32).astype(bf16)
    logs = all_log[...].reshape(rows, LANES)
    high = logs.astype(bf16)
    rest = logs - high.astype(f32)
    middle = rest.astype(bf16)
    low = (rest - middle.astype(f32)).astype(bf16)
    ordered = sum(jnp.dot(from_class, x, preferred_element_type=f32) for x in (high, middle, low))
    for j in range(rows // LANES):
        block = slice(j * LANES, (j + 1) * LANES)
        total_ref[:, block] = jnp.transpose(ordered[block])[:heads]

    def product(q):
        return jnp.dot(at[q].reshape(rows, lw), wo[q], preferred_element_type=f32)

    result = product(p)
    forward(order[1])
    w_sends[0].wait_recv()
    for k in range(n):
        gc[k].wait_recv()
    result += product(core)
    for copy in wf:
        copy.wait_recv()
    forward(order[2])
    result += product(xp)
    for k in range(n):
        gf[k].wait_recv()
    result += product(diag)
    mixed_ref[...] = jnp.dot(from_class, result.astype(bf16), preferred_element_type=f32).astype(bf16)
    for copy in sends:
        copy.wait_send()

    @pl.when(s < n - 1)
    def _():
        halo_send.wait_send()


def local_by_class(hidden, norm_gain, w_query, w_key, w_value, query_gain, key_gain, w_out):
    n = MIDDLE_DILATION
    rows, width = hidden.shape
    heads, hd = query_gain.shape
    lw = heads * hd
    sub = rows // n
    halo_sub = KEYS_BEHIND // n
    bf16, f32 = jnp.bfloat16, jnp.float32
    table = jnp.asarray(rotary_table(n, sub, hd))
    vmem = pl.BlockSpec(memory_space=pltpu.VMEM)
    anyspace = pl.BlockSpec(memory_space=pl.ANY)
    dma = pltpu.SemaphoreType.DMA
    mixed, total = pl.pallas_call(
        class_kernel,
        out_shape=(
            pltpu.VMEM((rows, w_out.shape[1] // 4), bf16),
            pltpu.VMEM((heads, rows), f32),
        ),
        in_specs=[anyspace] * 9,
        out_specs=(vmem, vmem),
        scratch_shapes=[
            pltpu.VMEM((rows, width), bf16),
            pltpu.VMEM((4 * width // LANES, LANES), bf16),
            pltpu.VMEM((heads, hd), f32),
            pltpu.VMEM((heads, hd), f32),
            pltpu.VMEM((4, n, sub, width), bf16),
            pltpu.VMEM((4, n, sub, width), bf16),
            pltpu.VMEM((4 * width, 3 * lw), bf16),
            pltpu.VMEM((4, lw, width), bf16),
            pltpu.VMEM((n, sub, 2 * hd), f32),
            pltpu.VMEM((n, sub, 2 * hd), f32),
            pltpu.VMEM((rows, 3 * lw), f32),
            pltpu.VMEM((n, sub, 3 * lw), f32),
            pltpu.VMEM((n, sub, lw), bf16),
            pltpu.VMEM((n, sub, 2 * lw), bf16),
            pltpu.VMEM((n, sub, 2 * lw), bf16),
            pltpu.VMEM((n, sub, lw), bf16),
            pltpu.VMEM((n, halo_sub, 2 * lw), bf16),
            pltpu.VMEM((heads, n, sub, hd), bf16),
            pltpu.VMEM((n, 8, LANES), f32),
            pltpu.VMEM((heads, n, sub, hd), bf16),
            pltpu.VMEM((n, 8, LANES), f32),
            pltpu.VMEM((heads, n, sub, hd), f32),
            pltpu.VMEM((n, sub, LANES), f32),
            pltpu.VMEM((n, sub, LANES), f32),
            pltpu.VMEM((4, n, sub, lw), bf16),
            pltpu.VMEM((4, 1, width), f32),
            dma((10,)),
            dma((n,)), dma((n,)),
            dma((n,)), dma((n,)), dma, dma, dma((n,)), dma((n,)),
            dma((n,)), dma((n,)), dma((n,)), dma((n,)), dma((n,)), dma((n,)),
            dma((3,)), dma((3,)), dma((2,)), dma((2,)),
            dma, dma,
            dma((heads, n)), dma((heads, n)), dma((n,)), dma((n,)),
            dma((n,)), dma((n,)), dma((n,)), dma((n,)), dma((n,)), dma((n,)),
        ],
        compiler_params=pltpu.CompilerParams(
            collective_id=0, has_side_effects=True, vmem_limit_bytes=60 * 1024 * 1024
        ),
    )(
        hidden, norm_gain.reshape(-1, LANES), query_gain, key_gain,
        w_query, w_key, w_value, w_out, table,
    )
    return mixed, total.T


def solution(mesh):
    split = (mesh.shape["grp"], mesh.shape["sp"], mesh.shape["tp"]) == (2, MIDDLE_DILATION, 4)
    chosen = local_by_class if split else local
    placed = (
        P(("grp", "sp"), "tp"),
        P(),
        P(None, "tp"),
        P(None, "tp"),
        P(None, "tp"),
        P("tp", None),
        P("tp", None),
        P("tp", None),
    )
    return jax.shard_map(
        chosen,
        mesh=mesh,
        in_specs=placed,
        out_specs=(P(("grp", "sp"), "tp"), P(("grp", "sp"), "tp")),
        check_vma=False,
    )
```

```python
import functools
import math

import jax
import jax.numpy as jnp
import numpy as np
from jax import lax
from jax.experimental import pallas as pl
from jax.experimental.pallas import tpu as pltpu
from jax.sharding import PartitionSpec as P

D = 2048
KEYS_BEHIND = 128
MIDDLE_DILATION = 4
WIDEST_DILATION = 16


EPSILON = 1e-06
ROTARY_BASE = 500000.0


def from_behind(value, axis, steps):
    count = lax.axis_size(axis)
    initial, last = (max(0, -steps), min(count, count - steps))
    return lax.ppermute(value, axis, [(source, source + steps) for source in range(initial, last)])


def rotate(values, positions):
    head_width = values.shape[-1]
    inverse = ROTARY_BASE ** (-jnp.arange(0, head_width, 2, dtype=jnp.float32) / head_width)
    angles = positions[:, None] * inverse[None, :]
    cosine = jnp.cos(angles)[:, None, :]
    sine = jnp.sin(angles)[:, None, :]
    half_width = head_width // 2
    first_half = values[..., :half_width]
    second_half = values[..., half_width:]
    return jnp.concatenate(
        [first_half * cosine - second_half * sine, second_half * cosine + first_half * sine],
        axis=-1,
    )


def head_norm(values, gains):
    normed = values * lax.rsqrt(jnp.mean(values * values, axis=-1, keepdims=True) + EPSILON)
    return normed * gains[None, :, :]


def earlier_pairs(own_pair, token_rows):
    distant_shards = (KEYS_BEHIND * WIDEST_DILATION + token_rows - 1) // token_rows
    pieces = [own_pair]
    for distance in range(1, distant_shards + 1):
        pieces.insert(0, from_behind(own_pair, "sp", distance))
    buffer = jnp.concatenate(pieces, axis=1)
    return buffer


def local_branch(query, key_rows, value_rows, dilation_step, first_pos):
    token_rows, head_count, head_width = query.shape
    reach_rows = KEYS_BEHIND * dilation_step
    buffer_rows = key_rows.shape[0]
    class_rows = token_rows // dilation_step
    class_keys = class_rows + KEYS_BEHIND
    window_start = buffer_rows - token_rows - reach_rows
    key_window = key_rows[window_start:]
    value_window = value_rows[window_start:]
    query_class = query.reshape(class_rows, dilation_step, head_count, head_width).transpose(
        1, 0, 2, 3
    )
    key_class = key_window.reshape(class_keys, dilation_step, head_count, head_width).transpose(
        1, 0, 2, 3
    )
    value_class = value_window.reshape(class_keys, dilation_step, head_count, head_width).transpose(
        1, 0, 2, 3
    )
    block_rows = math.gcd(class_rows, KEYS_BEHIND) if class_rows > KEYS_BEHIND else class_rows
    block_count = class_rows // block_rows
    query_blocks = query_class.reshape(
        dilation_step, block_count, block_rows, head_count, head_width
    )
    key_blocks = jnp.stack(
        [
            key_class[:, number * block_rows : number * block_rows + block_rows + KEYS_BEHIND]
            for number in range(block_count)
        ],
        axis=1,
    )
    value_blocks = jnp.stack(
        [
            value_class[:, number * block_rows : number * block_rows + block_rows + KEYS_BEHIND]
            for number in range(block_count)
        ],
        axis=1,
    )
    scores = jnp.einsum(
        "rnqhd,rnkhd->rnhqk", query_blocks, key_blocks, preferred_element_type=jnp.float32
    ) * head_width ** (-0.5)
    row_index = jnp.arange(block_rows, dtype=jnp.int32)[:, None]
    col_index = jnp.arange(block_rows + KEYS_BEHIND, dtype=jnp.int32)[None, :]
    distance = KEYS_BEHIND + row_index - col_index
    in_band = (distance >= 0) & (distance <= KEYS_BEHIND)
    class_index = jnp.arange(block_count, dtype=jnp.int32)[:, None] * block_rows + col_index
    residue = jnp.arange(dilation_step, dtype=jnp.int32)[:, None, None]
    key_position = first_pos - reach_rows + class_index[None] * dilation_step + residue
    allowed = in_band[None, None, None, :, :] & (key_position >= 0)[:, :, None, None, :]
    scores = jnp.where(allowed, scores, -jnp.inf)
    row_max = jnp.max(scores, axis=-1, keepdims=True)
    weights = jnp.exp(scores - row_max)
    weight_sum = jnp.sum(weights, axis=-1)
    weighted = jnp.einsum(
        "rnhqk,rnkhd->rnqhd",
        weights.astype(jnp.bfloat16),
        value_blocks,
        preferred_element_type=jnp.float32,
    )
    branch_out = weighted / jnp.transpose(weight_sum, (0, 1, 3, 2))[..., None]
    branch_out = branch_out.reshape(dilation_step, class_rows, head_count, head_width).transpose(
        1, 0, 2, 3
    )
    branch_out = branch_out.reshape(token_rows, head_count, head_width)
    log_sum = jnp.transpose(row_max[..., 0] + jnp.log(weight_sum), (0, 1, 3, 2))
    log_sum = (
        log_sum.reshape(dilation_step, class_rows, head_count)
        .transpose(1, 0, 2)
        .reshape(token_rows, head_count)
    )
    return (branch_out, log_sum)


def local(hidden, norm_gain, w_query, w_key, w_value, query_gain, key_gain, w_out):
    token_rows = hidden.shape[0]
    local_width = w_query.shape[1]
    head_count = query_gain.shape[0]
    head_width = query_gain.shape[1]
    gain_full = norm_gain.astype(jnp.float32)
    raw_piece = lax.all_gather(hidden, "tp", axis=1, tiled=True).astype(jnp.float32)
    scaled = (raw_piece * gain_full[None, :]).astype(jnp.bfloat16)

    def add_product(weight):
        return jnp.dot(scaled, weight, preferred_element_type=jnp.float32)

    query_raw = add_product(w_query)
    key_raw = add_product(w_key)
    value_raw = add_product(w_value)
    squares = jnp.sum(raw_piece * raw_piece, axis=1)
    row_scale = lax.rsqrt(squares / D + EPSILON)[:, None]
    first_pos = lax.axis_index("sp") * token_rows
    positions = (jnp.arange(token_rows, dtype=jnp.int32) + first_pos).astype(jnp.float32)
    query = rotate(
        head_norm((query_raw * row_scale).reshape(token_rows, head_count, head_width), query_gain),
        positions,
    ).astype(jnp.bfloat16)
    key_now = rotate(
        head_norm((key_raw * row_scale).reshape(token_rows, head_count, head_width), key_gain),
        positions,
    ).astype(jnp.bfloat16)
    value_now = (value_raw * row_scale).astype(jnp.bfloat16)
    own_pair = jnp.stack([key_now.reshape(token_rows, local_width), value_now], axis=0)
    buffer = earlier_pairs(own_pair, token_rows)
    key_rows = buffer[0].reshape(-1, head_count, head_width)
    value_rows = buffer[1].reshape(-1, head_count, head_width)
    branch_outs = []
    branch_logs = []
    for dilation_step in (1, MIDDLE_DILATION, WIDEST_DILATION):
        branch_out, log_sum = local_branch(query, key_rows, value_rows, dilation_step, first_pos)
        branch_outs.append(branch_out)
        branch_logs.append(log_sum)
    stacked_logs = jnp.stack(branch_logs, axis=0)
    peak = jnp.max(stacked_logs, axis=0)
    log_total = peak + jnp.log(jnp.sum(jnp.exp(stacked_logs - peak[None]), axis=0))
    shares = jnp.exp(stacked_logs - log_total[None])
    attended = jnp.sum(shares[..., None] * jnp.stack(branch_outs, axis=0), axis=0)
    attended = attended.astype(jnp.bfloat16).reshape(token_rows, local_width)
    column_block = lax.all_to_all(w_out, "tp", split_axis=1, concat_axis=0, tiled=True)
    mixed = jnp.dot(
        lax.all_gather(attended, "tp", axis=1, tiled=True),
        column_block,
        preferred_element_type=jnp.float32,
    )
    return (mixed.astype(jnp.bfloat16), log_total)


MESH = pl.DeviceIdType.MESH
LANES = 128


def rotary_table(classes, rows, head_width):
    inverse = (ROTARY_BASE ** (-np.arange(0, head_width, 2, dtype=np.float64) / head_width)).astype(np.float32)
    positions = np.arange(classes * classes * rows, dtype=np.float32)
    angles = (positions[:, None] * inverse[None, :]).astype(np.float64)
    cosine, sine = np.cos(angles), np.sin(angles)
    table = np.concatenate([cosine, cosine, -sine, sine], axis=1).astype(np.float32)
    return table.reshape(classes, rows, classes, 2 * head_width).transpose(0, 2, 1, 3)


def class_kernel(
    hid_ref, gain_ref, qgain_ref, kgain_ref, wq_ref, wk_ref, wv_ref, wo_ref, table_ref,
    mixed_ref, total_ref,
    hid, gain_in, qgain, kgain, hb, hc, wall, wo, tb, tc, acc_b, acc_c, q_b, kv_b, kv_c, q_c,
    halo, oc, lsend, ro, rl, near_out, near_log, all_log, at, gain, drain,
    loc, sent, zr, axr, acr, afr, cxr, ccr, cfr, wor, wfr, hs, hr, rr, lr, gxr, gcr, gfr,
):
    f32, bf16 = jnp.float32, jnp.bfloat16
    g, s, p = lax.axis_index("grp"), lax.axis_index("sp"), lax.axis_index("tp")
    n = MIDDLE_DILATION
    rows, width = hid_ref.shape
    sub = rows // n
    heads, hd = qgain_ref.shape
    lw = heads * hd
    halo_sub = halo.shape[1]
    halo_rows = n * halo_sub
    core = p + 1 - 2 * lax.rem(p, 2)
    xp = lax.rem(p + 2, 4)
    diag = lax.rem(core + 2, 4)
    order = (1, 2, 3)
    block_of = [s, s + 1 - 2 * lax.rem(s, 2), 2 - s // 2, 3 - 3 * (s // 2)]

    def copy_to(axis, src, dst, ss, sr, q):
        return pltpu.make_async_remote_copy(
            src_ref=src, dst_ref=dst, send_sem=ss, recv_sem=sr, device_id={axis: q}, device_id_type=MESH
        )

    tp_copy = functools.partial(copy_to, "tp")
    sp_copy = functools.partial(copy_to, "sp")
    load_hid = pltpu.make_async_copy(hid_ref, hid, loc.at[1])
    load_hid.start()
    barrier = pltpu.get_barrier_semaphore()
    for q in (core, xp, diag):
        pl.semaphore_signal(barrier, inc=1, device_id={"tp": q}, device_id_type=MESH)
    for k in range(1, n):
        pl.semaphore_signal(barrier, inc=1, device_id={"sp": lax.rem(s + k, n)}, device_id_type=MESH)
    pl.semaphore_signal(barrier, inc=1, device_id={"grp": 1 - g}, device_id_type=MESH)
    loads = [
        pltpu.make_async_copy(gain_ref, gain_in, loc.at[0]),
        pltpu.make_async_copy(qgain_ref, qgain, loc.at[2]),
        pltpu.make_async_copy(kgain_ref, kgain, loc.at[3]),
        pltpu.make_async_copy(wq_ref, wall.at[:, pl.ds(0, lw)], loc.at[4]),
        pltpu.make_async_copy(wk_ref, wall.at[:, pl.ds(lw, lw)], loc.at[5]),
        pltpu.make_async_copy(wv_ref, wall.at[:, pl.ds(2 * lw, lw)], loc.at[6]),
        pltpu.make_async_copy(table_ref.at[s], tb, loc.at[7]),
        pltpu.make_async_copy(table_ref.at[:, s], tc, loc.at[8]),
        pltpu.make_async_copy(
            wo_ref.at[:, pl.ds(pl.multiple_of(p * width, LANES), width)], wo.at[p], loc.at[9]
        ),
    ]
    for load in loads:
        load.start()

    def iota(shape, dim):
        return lax.broadcasted_iota(jnp.int32, shape, dim)

    def row_of(r, part):
        return n * lax.rem(r, part) + r // part

    square = (rows, rows)
    to_class = (row_of(iota(square, 0), sub) == iota(square, 1)).astype(f32).astype(bf16)
    load_hid.wait()
    permuted = jnp.dot(to_class, hid[...], preferred_element_type=f32).astype(bf16)
    hb[p] = permuted.reshape(n, sub, width)
    pl.semaphore_wait(barrier, 3 + n)

    sends = []

    def go(copy):
        copy.start()
        sends.append(math.prod(copy.src_ref.shape) * copy.src_ref.dtype.itemsize)
        return copy

    for k in order:
        to = block_of[k]
        go(sp_copy(hb.at[p, to], hc.at[p, s], sent, zr.at[s], to))
    piece_of = [lax.rem(s + k, n) for k in range(n)]
    ax = [go(tp_copy(hb.at[p, i], hb.at[p, i], sent, axr.at[j], xp)) for j, i in enumerate(piece_of)]
    ac = go(tp_copy(hb.at[p], hb.at[p], sent, acr, core))

    cx, cc, cf = {}, {}, {}

    def spread(k):
        piece = hc.at[p, block_of[k]]
        cx[k] = go(tp_copy(piece, piece, sent, cxr.at[k], xp))
        cc[k] = go(tp_copy(piece, piece, sent, ccr.at[k], core))

    for load in loads:
        load.wait()
    flat_gain = gain_in[...].astype(f32)
    for j in range(flat_gain.shape[0]):
        each = width // LANES
        gain[j // each, :, (j % each) * LANES : (j % each + 1) * LANES] = flat_gain[j : j + 1]

    def chunk(raw, q):
        raw = raw.astype(f32)
        scaled = (raw * gain[q]).astype(bf16)
        w = wall[pl.ds(pl.multiple_of(q * width, LANES), width), :]
        return jnp.dot(scaled, w, preferred_element_type=f32), jnp.sum(raw * raw, axis=1, keepdims=True)

    def chunk_b(q):
        return chunk(hb[q].reshape(rows, width), q)

    acc_b[...], sq_b = chunk_b(p)
    ac.wait_recv()
    prod, more = chunk_b(core)
    acc_b[...] += prod
    sq_b += more

    for j, i in enumerate(piece_of):
        ax[j].wait_recv()
        go(tp_copy(hb.at[xp, i], hb.at[xp, i], sent, afr, core))
        if j >= 1:
            source = block_of[order[j - 1]]
            sp_copy(hb.at[p, source], hc.at[p, source], sent, zr.at[source], source).wait_recv()
            spread(order[j - 1])
    half = lw // 2
    mine = pl.ds(pl.multiple_of(g * half, 8), half)
    w_sends = [
        go(tp_copy(wo_ref.at[:, pl.ds(pl.multiple_of(core * width, LANES), width)], wo.at[p], sent, wor.at[0], core))
    ]
    for j, q in ((1, xp), (2, diag)):
        w_sends.append(go(tp_copy(
            wo_ref.at[mine, pl.ds(pl.multiple_of(q * width, LANES), width)], wo.at[p, mine], sent, wor.at[j], q
        )))

    prod, more = chunk_b(xp)
    acc_b[...] += prod
    sq_b += more
    def pieces(ks, q):
        return chunk(jnp.concatenate([hb[q, s] if k == 0 else hc[q, block_of[k]] for k in ks], axis=0), q)

    def close_pieces(ks):
        for k in ks:
            if k != 0:
                cc[k].wait_recv()
        first, squares = pieces(ks, p)
        prod, more = pieces(ks, core)
        return first + prod, squares + more

    def cross(k):
        cx[k].wait_recv()
        piece = hc.at[xp, block_of[k]]
        cf[k] = go(tp_copy(piece, piece, sent, cfr.at[k], core))

    acc_c[0], sq_0 = close_pieces((0, 1))
    cross(1)
    tp_copy(hb.at[diag], hb.at[diag], sent, afr, core).wait_recv()
    prod, more = chunk_b(diag)
    sq_b += more

    def finish(acc, sq, table, put_q, put_kv):
        raw = acc * lax.rsqrt(sq / (width * 4) + EPSILON)
        cosine, sine = table[:, :hd], table[:, hd:]
        for h in range(heads):
            for start, gains, put in ((0, qgain, put_q), (lw, kgain, put_kv)):
                x = raw[:, start + h * hd : start + (h + 1) * hd]
                x = x * lax.rsqrt(jnp.mean(x * x, axis=-1, keepdims=True) + EPSILON)
                x = x * gains[pl.ds(h, 1), :]
                x = x * cosine + pltpu.roll(x, hd // 2, 1) * sine
                put(slice(h * hd, (h + 1) * hd), x.astype(bf16))
        put_kv(slice(lw, 2 * lw), raw[:, 2 * lw :].astype(bf16))

    def put_all(ref):
        def put(cols, x):
            ref[:, :, cols] = x.reshape(n, sub, x.shape[1])
        return put

    def put_block(ref, b):
        def put(cols, x):
            ref[b, :, cols] = x
        return put

    finish(acc_b[...] + prod, sq_b, tb[...].reshape(rows, 2 * hd), put_all(q_b), put_all(kv_b))
    halo_send = sp_copy(kv_b.at[:, pl.ds(sub - halo_sub, halo_sub), :], halo, hs, hr, lax.rem(s + 1, n))

    @pl.when(s < n - 1)
    def _():
        halo_send.start()

    @pl.when(s == 0)
    def _():
        halo[...] = jnp.zeros_like(halo)

    def finish_c(ks, acc, sq):
        prod, more = pieces(ks, diag)
        acc, sq = acc + prod, sq + more
        for j, k in enumerate(ks):
            part, b = slice(j * sub, (j + 1) * sub), block_of[k]
            finish(acc[part], sq[part], tc[b], put_block(q_c, b), put_block(kv_c, b))

    prod, more = pieces((0, 1), xp)
    acc_c[0] += prod
    sq_0 += more
    cf[1].wait_recv()
    finish_c((0, 1), acc_c[0], sq_0)
    cross(2)
    acc_c[1], sq_1 = close_pieces((2, 3))
    cross(3)
    prod, more = pieces((2, 3), xp)
    acc_c[1] += prod
    sq_1 += more
    cf[2].wait_recv()
    cf[3].wait_recv()
    finish_c((2, 3), acc_c[1], sq_1)

    def attend(q, k, v, bias):
        score = lax.dot_general(q, k, (((1,), (1,)), ((), ())), preferred_element_type=f32)
        score = score * hd ** (-0.5) + bias
        top = jnp.max(score, axis=-1, keepdims=True)
        weight = jnp.exp(score - top)
        total = jnp.sum(weight, axis=-1, keepdims=True)
        out = jnp.dot(weight.astype(bf16), v, preferred_element_type=f32) / total
        return out, top + jnp.log(total)

    behind = iota(square, 0) - iota(square, 1)
    stride = WIDEST_DILATION // n
    near = (behind >= 0) & (behind <= KEYS_BEHIND)
    far = (behind >= 0) & (behind <= KEYS_BEHIND * stride) & ((behind + rows * stride) % stride == 0)
    bias_c = jnp.where(
        near & far, math.log(2.0), jnp.where(near | far, 0.0, -jnp.inf)
    ).astype(f32)
    lane = iota((rows, LANES), 1)
    logs = jnp.zeros((rows, LANES), f32)
    for h in range(heads):
        cols = slice(h * hd, (h + 1) * hd)
        vcols = slice(lw + h * hd, lw + (h + 1) * hd)
        out, lse = attend(
            q_c[:, :, cols].reshape(rows, hd), kv_c[:, :, cols].reshape(rows, hd),
            kv_c[:, :, vcols].reshape(rows, hd), bias_c,
        )
        oc[h] = out.astype(bf16).reshape(n, sub, hd)
        logs = jnp.where(lane == h, lse, logs)
        for k in order[::-1]:
            to = block_of[k]
            go(sp_copy(oc.at[h, to], ro.at[s, h], sent, rr.at[s], to))
    pad = LANES - sub
    for b in range(n):
        part = jnp.concatenate([logs[b * sub : (b + 1) * sub], jnp.zeros((pad, LANES), f32)], axis=0)
        lsend[b] = jnp.transpose(part)[:8]
    for k in order[::-1]:
        to = block_of[k]
        go(sp_copy(lsend.at[to], rl.at[s], sent, lr.at[s], to))

    @pl.when(s > 0)
    def _():
        halo_send.wait_recv()

    total_keys = rows + halo_rows
    wide = (rows, total_keys)
    key = iota(wide, 1)
    key_row = jnp.where(key < rows, row_of(key, sub), row_of(key - rows, halo_sub) - halo_rows)
    behind = row_of(iota(wide, 0), sub) - key_row
    ok = (behind >= 0) & (behind <= KEYS_BEHIND) & (key_row + s * rows >= 0)
    bias_b = jnp.where(ok, 0.0, -jnp.inf).astype(f32)
    logs = jnp.zeros((rows, LANES), f32)
    for h in range(heads):
        cols = slice(h * hd, (h + 1) * hd)
        vcols = slice(lw + h * hd, lw + (h + 1) * hd)
        out, lse = attend(
            q_b[:, :, cols].reshape(rows, hd),
            jnp.concatenate([kv_b[:, :, cols].reshape(rows, hd), halo[:, :, cols].reshape(halo_rows, hd)], axis=0),
            jnp.concatenate([kv_b[:, :, vcols].reshape(rows, hd), halo[:, :, vcols].reshape(halo_rows, hd)], axis=0),
            bias_b,
        )
        near_out[h] = out.reshape(n, sub, hd)
        logs = jnp.where(lane == h, lse, logs)
    near_log[...] = logs.reshape(n, sub, LANES)

    gx, gc, gf = {}, {}, {}

    def merge(k):
        b = block_of[k]
        received = lsend[s] if k == 0 else rl[b]
        far_log = jnp.transpose(jnp.concatenate([received, jnp.zeros((LANES - 8, LANES), f32)], axis=0))[:sub]
        logs = jnp.zeros((sub, LANES), f32)
        for h in range(heads):
            lse = near_log[b][:, h : h + 1]
            far_lse = far_log[:, h : h + 1]
            far_out = (oc[h, s] if k == 0 else ro[b, h]).astype(f32)
            top = jnp.maximum(lse, far_lse)
            e_near, e_far = jnp.exp(lse - top), jnp.exp(far_lse - top)
            both = e_near + e_far
            logs = jnp.where(lane[:sub] == h, top + jnp.log(both), logs)
            at[p, b, :, h * hd : (h + 1) * hd] = ((e_near * near_out[h, b] + e_far * far_out) / both).astype(bf16)
        all_log[b] = logs
        piece = at.at[p, b]
        gx[k] = go(tp_copy(piece, piece, sent, gxr.at[k], xp))
        gc[k] = go(tp_copy(piece, piece, sent, gcr, core))

    def forward(k):
        gx[k].wait_recv()
        piece = at.at[xp, block_of[k]]
        gf[k] = go(tp_copy(piece, piece, sent, gfr, core))

    merge(0)
    wf = []
    for j, q in ((1, xp), (2, diag)):
        w_sends[j].wait_recv()
        wf.append(go(copy_to("grp", wo.at[q, mine], wo.at[q, mine], sent, wfr.at[j - 1], 1 - g)))
    for k, ready in zip(order, (None, 0, order[0])):
        b = block_of[k]
        sp_copy(ro.at[b], ro.at[b], sent, rr.at[b], b).wait_recv()
        sp_copy(rl.at[b], rl.at[b], sent, lr.at[b], b).wait_recv()
        merge(k)
        if ready is not None:
            forward(ready)
    from_class = (iota(square, 0) == row_of(iota(square, 1), sub)).astype(f32).astype(bf16)
    logs = all_log[...].reshape(rows, LANES)
    high = logs.astype(bf16)
    rest = logs - high.astype(f32)
    middle = rest.astype(bf16)
    low = (rest - middle.astype(f32)).astype(bf16)
    ordered = sum(jnp.dot(from_class, x, preferred_element_type=f32) for x in (high, middle, low))
    for j in range(rows // LANES):
        block = slice(j * LANES, (j + 1) * LANES)
        total_ref[:, block] = jnp.transpose(ordered[block])[:heads]

    def product(q):
        return jnp.dot(at[q].reshape(rows, lw), wo[q], preferred_element_type=f32)

    result = product(p)
    forward(order[1])
    w_sends[0].wait_recv()
    tp_copy(at.at[core], at.at[core], sent, gcr, core).wait_recv()
    result += product(core)
    for copy in wf:
        copy.wait_recv()
    forward(order[2])
    result += product(xp)
    tp_copy(at.at[diag], at.at[diag], sent, gfr, core).wait_recv()
    result += product(diag)
    mixed_ref[...] = jnp.dot(from_class, result.astype(bf16), preferred_element_type=f32).astype(bf16)
    assert sum(sends) == drain.shape[0] * LANES * 4
    tp_copy(drain, drain, sent, acr, core).wait_send()

    @pl.when(s < n - 1)
    def _():
        halo_send.wait_send()


def local_by_class(hidden, norm_gain, w_query, w_key, w_value, query_gain, key_gain, w_out):
    n = MIDDLE_DILATION
    rows, width = hidden.shape
    heads, hd = query_gain.shape
    lw = heads * hd
    sub = rows // n
    halo_sub = KEYS_BEHIND // n
    bf16, f32 = jnp.bfloat16, jnp.float32
    table = jnp.asarray(rotary_table(n, sub, hd))
    sent_bytes = 2 * (24 * sub * width + 3 * lw * width + 3 * sub * lw + 12 * sub * lw) + 3 * 8 * LANES * 4
    vmem = pl.BlockSpec(memory_space=pltpu.VMEM)
    anyspace = pl.BlockSpec(memory_space=pl.ANY)
    dma = pltpu.SemaphoreType.DMA
    mixed, total = pl.pallas_call(
        class_kernel,
        out_shape=(
            pltpu.VMEM((rows, w_out.shape[1] // 4), bf16),
            pltpu.VMEM((heads, rows), f32),
        ),
        in_specs=[anyspace] * 9,
        out_specs=(vmem, vmem),
        scratch_shapes=[
            pltpu.VMEM((rows, width), bf16),
            pltpu.VMEM((4 * width // LANES, LANES), bf16),
            pltpu.VMEM((heads, hd), f32),
            pltpu.VMEM((heads, hd), f32),
            pltpu.VMEM((4, n, sub, width), bf16),
            pltpu.VMEM((4, n, sub, width), bf16),
            pltpu.VMEM((4 * width, 3 * lw), bf16),
            pltpu.VMEM((4, lw, width), bf16),
            pltpu.VMEM((n, sub, 2 * hd), f32),
            pltpu.VMEM((n, sub, 2 * hd), f32),
            pltpu.VMEM((rows, 3 * lw), f32),
            pltpu.VMEM((2, 2 * sub, 3 * lw), f32),
            pltpu.VMEM((n, sub, lw), bf16),
            pltpu.VMEM((n, sub, 2 * lw), bf16),
            pltpu.VMEM((n, sub, 2 * lw), bf16),
            pltpu.VMEM((n, sub, lw), bf16),
            pltpu.VMEM((n, halo_sub, 2 * lw), bf16),
            pltpu.VMEM((heads, n, sub, hd), bf16),
            pltpu.VMEM((n, 8, LANES), f32),
            pltpu.VMEM((n, heads, sub, hd), bf16),
            pltpu.VMEM((n, 8, LANES), f32),
            pltpu.VMEM((heads, n, sub, hd), f32),
            pltpu.VMEM((n, sub, LANES), f32),
            pltpu.VMEM((n, sub, LANES), f32),
            pltpu.VMEM((4, n, sub, lw), bf16),
            pltpu.VMEM((4, 1, width), f32),
            pltpu.VMEM((sent_bytes // (4 * LANES), LANES), f32),
            dma((10,)), dma, dma((n,)), dma((n,)), dma, dma, dma((n,)), dma((n,)), dma((n,)),
            dma((3,)), dma((2,)), dma, dma, dma((n,)), dma((n,)), dma((n,)), dma, dma,
        ],
        compiler_params=pltpu.CompilerParams(
            collective_id=0, has_side_effects=True, vmem_limit_bytes=60 * 1024 * 1024
        ),
    )(
        hidden, norm_gain.reshape(-1, LANES), query_gain, key_gain,
        w_query, w_key, w_value, w_out, table,
    )
    return mixed, total.T


def solution(mesh):
    split = (mesh.shape["grp"], mesh.shape["sp"], mesh.shape["tp"]) == (2, MIDDLE_DILATION, 4)
    chosen = local_by_class if split else local
    placed = (
        P(("grp", "sp"), "tp"),
        P(),
        P(None, "tp"),
        P(None, "tp"),
        P(None, "tp"),
        P("tp", None),
        P("tp", None),
        P("tp", None),
    )
    return jax.shard_map(
        chosen,
        mesh=mesh,
        in_specs=placed,
        out_specs=(P(("grp", "sp"), "tp"), P(("grp", "sp"), "tp")),
        check_vma=False,
    )
```
